32 devices in a mesh: sp: 16 (over z, y, core), tp: 2 (over x).
Axes of the slice: x: 2, y: 2, z: 4, core: 2. Of those that a mesh axis runs over, the one named last changes fastest.
Arguments:
- query_latent: bfloat16 [4096, 1024], P('sp'), may hold values from -6 to 6
- shared_latent: bfloat16 [4096, 512], P('sp'), may hold values from -25 to 25
- rotary_key: bfloat16 [4096, 64], P('sp'), may hold values from -300 to 300
- document_start: int32 [4096], P('sp'), may hold values from 0 to 4095, as said below
- query_gain: float32 [1024], replicated, may hold values from 0.1 to 1.9
- shared_gain: float32 [512], replicated, may hold values from 0.1 to 1.9
- content_weight: bfloat16 [1024, 2048], P(None, 'tp'), may hold values from -0.1875 to 0.1875
- rotary_weight: bfloat16 [1024, 1024], P(None, 'tp'), may hold values from -0.1875 to 0.1875
- key_weight: bfloat16 [512, 2048], P(None, 'tp'), may hold values from -0.25 to 0.25
- value_weight: bfloat16 [512, 2048], P(None, 'tp'), may hold values from -0.25 to 0.25
- output_weight: bfloat16 [2048, 4096], P('tp'), may hold values from -0.125 to 0.125
Outputs:
- mixed: bfloat16 [4096, 4096], P('sp')
The draws below stay inside these ranges and needn't reach their ends.
Inputs may be any that keep to these rules, and one draw needn't show every extreme that they name: `document_start`: each position holds the first position of its document; documents are runs of 1 to 1792 consecutive positions and one of them has exactly 1792; the values never fall.
All inputs are finite; a program needn't handle non-finite values.
Results may differ from the reference program's by a relative error of at most 0.038.
The reference program's roundings to bfloat16 on the way count: a program that leaves them out, or rounds other values in their place, can miss the bound.
Values may be sent and summed in bfloat16 or wider, within the bound.
No kernel may reach another device: no remote copies, remote signals or barrier semaphores. Data moves between devices by JAX's collectives and lax.ppermute only.
A program may use at most 64 MiB of HBM per device.

```python
import jax
import jax.numpy as jnp
from jax import lax

MODEL = 4096
HEADS = 16
CONTENT = 128
ROTARY = 64
VALUE_DIM = 128
QUERY_RANK = 1024
SHARED_RANK = 512
SPAN = 8
TOK_DEV = 256
TOKENS = 4096
DOC_MOST = 1792
HEADS_DEV = 8


def draw_shared_latent(key, part):
    first_key = jax.random.fold_in(key, 11)
    second_key = jax.random.fold_in(key, 12)
    blocks = TOKENS // TOK_DEV
    base = jnp.clip(jax.random.normal(first_key, (TOKENS, SHARED_RANK), jnp.float32), -6.0, 6.0)
    means = 0.8 * jnp.clip(jax.random.normal(second_key, (blocks, SHARED_RANK), jnp.float32), -6.0, 6.0)
    result = base + jnp.repeat(means, TOK_DEV, axis=0)
    return jnp.clip(result, -25.0, 25.0).astype(jnp.bfloat16)


def draw_rotary_key(key, part):
    first_key = jax.random.fold_in(key, 21)
    result = jnp.clip(jax.random.normal(first_key, (TOKENS, ROTARY), jnp.float32), -6.0, 6.0)
    return jnp.clip(result, -300.0, 300.0).astype(jnp.bfloat16)


def draw_document_start(key, part):
    first_key = jax.random.fold_in(key, 31)
    second_key = jax.random.fold_in(key, 32)
    positions = jnp.arange(TOKENS, dtype=jnp.int32)
    lengths = jax.random.randint(first_key, (TOKENS,), 1, DOC_MOST + 1, dtype=jnp.int32)
    opening = jax.random.randint(second_key, (), 1, TOK_DEV, dtype=jnp.int32)
    lengths = jnp.where(positions == 0, opening, jnp.where(positions == 1, DOC_MOST, lengths))
    starts = jnp.cumsum(lengths).astype(jnp.int32) - lengths
    document = jnp.searchsorted(starts, positions, side='right') - 1
    result = starts[document].astype(jnp.int32)
    return jnp.where(positions == TOKENS - 1, positions, result).astype(jnp.int32)


def block_scale(key, shape, shards, low, largest):
    factor_of, own = 1.0, jax.random.fold_in(key, 6)
    for position, shards_of in shards:
        draws = jnp.exp(jax.random.uniform(jax.random.fold_in(own, position), (shards_of,), jnp.float32, low / len(shards), largest / len(shards)))
        factor_of = factor_of * jnp.repeat(draws, shape[position] // shards_of).reshape([-1 if axis == position else 1 for axis in range(len(shape))])
    return factor_of


def bell_draw(rng, extent, scale, bound, pieces=(), held_as=jnp.bfloat16):
    values = jax.random.normal(rng, extent, jnp.float32) * scale
    if len(pieces) > 0:
        values = block_scale(rng, extent, pieces, -0.22, 0.18) * values
    return jnp.clip(values, min=-bound, max=bound).astype(held_as)


def setup_inputs(seed: int = 0) -> dict:
    arg_keys = jax.random.split(jax.random.key(seed), 12)
    return {
        "query_latent": bell_draw(arg_keys[0], (TOKENS, QUERY_RANK), 1.0, 6.0, ((0, 16),)),
        "shared_latent": draw_shared_latent(jax.random.fold_in(arg_keys[11], 71), 0),
        "rotary_key": draw_rotary_key(jax.random.fold_in(arg_keys[11], 71), 0),
        "document_start": draw_document_start(jax.random.fold_in(arg_keys[11], 71), 0),
        "query_gain": jnp.clip(1.0 + 0.18 * jax.random.normal(arg_keys[4], (QUERY_RANK,), jnp.float32), 0.1, 1.9),
        "shared_gain": jnp.clip(1.0 + 0.18 * jax.random.normal(arg_keys[5], (SHARED_RANK,), jnp.float32), 0.1, 1.9),
        "content_weight": bell_draw(arg_keys[6], (QUERY_RANK, HEADS * CONTENT), QUERY_RANK ** -0.5, 0.1875, ((1, 2),)),
        "rotary_weight": bell_draw(arg_keys[7], (QUERY_RANK, HEADS * ROTARY), QUERY_RANK ** -0.5, 0.1875, ((1, 2),)),
        "key_weight": bell_draw(arg_keys[8], (SHARED_RANK, HEADS * CONTENT), SHARED_RANK ** -0.5, 0.25, ((1, 2),)),
        "value_weight": bell_draw(arg_keys[9], (SHARED_RANK, HEADS * VALUE_DIM), SHARED_RANK ** -0.5, 0.25, ((1, 2),)),
        "output_weight": bell_draw(arg_keys[10], (HEADS * VALUE_DIM, MODEL), (HEADS * VALUE_DIM) ** -0.5, 0.125, ((0, 2),)),
    }


norm_eps = 1e-06
rope_theta = 10000.0
masked_score = -1e+30

def rms_scale(latent, scaling):
    entries = latent.astype(jnp.float32)
    scaled = entries * lax.rsqrt(lax.optimization_barrier(jnp.mean(entries * entries, axis=-1, keepdims=True)) + norm_eps)
    return (scaled * scaling.astype(jnp.float32)).astype(jnp.bfloat16)

def rotate(entries, places):
    width = entries.shape[-1]
    halfway = width // 2
    frequency = 1.0 / rope_theta ** (jnp.arange(0, width, 2, dtype=jnp.float32) / width)
    angles = places.astype(jnp.float32)[:, None] * frequency[None, :]
    target = (angles.shape[0],) + (1,) * (entries.ndim - 2) + (halfway,)
    cosine_table = jnp.cos(angles).reshape(target)
    sine_table = jnp.sin(angles).reshape(target)
    leading = entries[..., :halfway]
    trailing = entries[..., halfway:]
    return jnp.concatenate([leading * cosine_table - trailing * sine_table, leading * sine_table + trailing * cosine_table], axis=-1)

def reference(query_latent, shared_latent, rotary_key, document_start, query_gain, shared_gain, content_weight, rotary_weight, key_weight, value_weight, output_weight):
    places = jnp.arange(TOKENS, dtype=jnp.int32)
    query_norm = rms_scale(query_latent, query_gain)
    shared_norm = rms_scale(shared_latent, shared_gain)
    key_turn = rotate(rotary_key.astype(jnp.float32), places).astype(jnp.bfloat16)
    query_content = jnp.dot(query_norm, content_weight, preferred_element_type=jnp.float32).astype(jnp.bfloat16).reshape(TOKENS, HEADS, CONTENT)
    query_raw = jnp.dot(query_norm, rotary_weight, preferred_element_type=jnp.float32).reshape(TOKENS, HEADS, ROTARY)
    query_turn = rotate(query_raw, places).astype(jnp.bfloat16)
    head_keys = jnp.dot(shared_norm, key_weight, preferred_element_type=jnp.float32).astype(jnp.bfloat16).reshape(TOKENS, HEADS, CONTENT)
    head_values = jnp.dot(shared_norm, value_weight, preferred_element_type=jnp.float32).astype(jnp.bfloat16).reshape(TOKENS, HEADS, VALUE_DIM)
    leading_pad = (SPAN - 1) * TOK_DEV
    window = SPAN * TOK_DEV
    padded_keys = jnp.pad(head_keys, ((leading_pad, 0), (0, 0), (0, 0)))
    padded_values = jnp.pad(head_values, ((leading_pad, 0), (0, 0), (0, 0)))
    padded_turn = jnp.pad(key_turn, ((leading_pad, 0), (0, 0)))
    score_scale = (CONTENT + ROTARY) ** (-0.5)

    def attend(block):
        opening = (block * TOK_DEV).astype(jnp.int32)
        block_content = lax.dynamic_slice_in_dim(query_content, opening, TOK_DEV, 0).astype(jnp.float32)
        block_turn = lax.dynamic_slice_in_dim(query_turn, opening, TOK_DEV, 0).astype(jnp.float32)
        block_starts = lax.dynamic_slice_in_dim(document_start, opening, TOK_DEV, 0)
        window_keys = lax.dynamic_slice_in_dim(padded_keys, opening, window, 0).astype(jnp.float32)
        window_values = lax.dynamic_slice_in_dim(padded_values, opening, window, 0).astype(jnp.float32)
        window_turn = lax.dynamic_slice_in_dim(padded_turn, opening, window, 0).astype(jnp.float32)
        key_places = opening - leading_pad + jnp.arange(window, dtype=jnp.int32)
        query_places = opening + jnp.arange(TOK_DEV, dtype=jnp.int32)
        scores = jnp.einsum('qhd,khd->hqk', block_content, window_keys) + jnp.einsum('qhr,kr->hqk', block_turn, window_turn)
        visible = (key_places[None, :] >= block_starts[:, None]) & (key_places[None, :] <= query_places[:, None])
        scores = jnp.where(visible[None], scores * score_scale, masked_score)
        highest = lax.optimization_barrier(jnp.max(scores, axis=-1, keepdims=True))
        weights = jnp.exp(scores - highest)
        denominator = lax.optimization_barrier(jnp.sum(weights, axis=-1))
        weights_low = weights.astype(jnp.bfloat16).astype(jnp.float32)
        summed = jnp.einsum('hqk,khd->qhd', weights_low, window_values)
        attended = summed / jnp.transpose(denominator)[:, :, None]
        return attended.astype(jnp.bfloat16).reshape(TOK_DEV, HEADS * VALUE_DIM)
    blocks = jnp.arange(TOKENS // TOK_DEV, dtype=jnp.int32)
    attended = lax.map(attend, blocks).reshape(TOKENS, HEADS * VALUE_DIM)
    group_width = HEADS_DEV * VALUE_DIM
    mixed = jnp.zeros((TOKENS, MODEL), jnp.float32)
    for group in range(HEADS // HEADS_DEV):
        columns = attended[:, group * group_width:(group + 1) * group_width]
        matching = output_weight[group * group_width:(group + 1) * group_width]
        group_term = jnp.dot(columns, matching, preferred_element_type=jnp.float32).astype(jnp.bfloat16)
        mixed = mixed + group_term.astype(jnp.float32)
    return mixed.astype(jnp.bfloat16)
```

```python
import functools

import jax
import jax.numpy as jnp
from jax import lax
from jax.experimental import pallas as pl
from jax.experimental.pallas import tpu as pltpu
from jax.sharding import PartitionSpec as P

CONTENT = 128
ROTARY = 64
VALUE_DIM = 128
SPAN = 8
GROUP = 4

norm_eps = 1e-06
rope_theta = 10000.0
masked_score = -1e30
LOG2E = 1.4426950408889634


def vmem():
    return pl.BlockSpec(memory_space=pltpu.VMEM)


def smem():
    return pl.BlockSpec(memory_space=pltpu.SMEM)


def normed(latent, gain):
    entries = latent.astype(jnp.float32)
    scale = lax.rsqrt(jnp.mean(entries * entries, axis=-1, keepdims=True) + norm_eps)
    return (entries * scale * gain).astype(jnp.bfloat16)


def swap_halves(x):
    width = x.shape[-1]
    half = ROTARY // 2
    lane = lax.broadcasted_iota(jnp.int32, x.shape, x.ndim - 1)
    ahead = pltpu.roll(x, width - half, x.ndim - 1)
    behind = pltpu.roll(x, half, x.ndim - 1)
    return jnp.where(lane % ROTARY < half, ahead, behind)


def pack_kernel(shared_ref, rotary_ref, gain_ref, cos_ref, sin_ref, out_ref):
    length, rank = shared_ref.shape
    out_ref[0:length, :] = normed(shared_ref[...], gain_ref[...])
    key = rotary_ref[...].astype(jnp.float32)
    key = jnp.concatenate([key, key], axis=-1)
    turned = key * cos_ref[...] + swap_halves(key) * sin_ref[...]
    rows = length * ROTARY // rank
    lane = lax.broadcasted_iota(jnp.int32, (rows, 2 * ROTARY), 1)
    for pair in range(rank // (2 * ROTARY)):
        low = turned[(2 * pair) * rows : (2 * pair + 1) * rows]
        high = turned[(2 * pair + 1) * rows : (2 * pair + 2) * rows]
        out_ref[length:, pair * 2 * ROTARY : (pair + 1) * 2 * ROTARY] = jnp.where(
            lane < ROTARY, low, high
        ).astype(jnp.bfloat16)


def query_kernel(latent_ref, gain_ref, content_ref, rotary_ref, cos_ref, sin_ref, out_ref):
    rows = normed(latent_ref[...], gain_ref[...])
    content = jnp.dot(rows, content_ref[...], preferred_element_type=jnp.float32)
    raw = jnp.dot(rows, rotary_ref[...], preferred_element_type=jnp.float32)
    lane = lax.broadcasted_iota(jnp.int32, (rows.shape[0], 2 * ROTARY), 1)
    for pair in range(out_ref.shape[0] // 2):
        piece = raw[:, pair * 2 * ROTARY : (pair + 1) * 2 * ROTARY]
        turned = piece * cos_ref[...] + swap_halves(piece) * sin_ref[...]
        for side in range(2):
            head = 2 * pair + side
            out_ref[head, :, 0:CONTENT] = content[
                :, head * CONTENT : (head + 1) * CONTENT
            ].astype(jnp.bfloat16)
            own = (lane < ROTARY) if side == 0 else (lane >= ROTARY)
            out_ref[head, :, CONTENT:] = jnp.where(own, turned, 0.0).astype(jnp.bfloat16)


def attend_kernel(places, axis, first, last, *refs):
    count = len(places)
    starts_smem, starts_ref, query_ref, key_ref, value_ref = refs[:5]
    blocks = refs[5 : 5 + count]
    refs = refs[5 + count :]
    if not first:
        old_stat, old_acc = refs[:2]
        refs = refs[2:]
    stat_ref, acc_ref, bias_ref, keys_ref, values_ref = refs
    heads = query_ref.shape[0]
    length = query_ref.shape[1]
    rank = key_ref.shape[0]
    me = lax.axis_index(axis)
    first_start = starts_smem[0]
    scale = (CONTENT + ROTARY) ** (-0.5) * LOG2E
    if not last:
        out_stat, out_acc = stat_ref, acc_ref
    if not first:
        stat_ref[...] = old_stat[...]
        acc_ref[...] = old_acc[...]

    def process(place_of, block_ref, own):
        block = place_of(me)

        def work():
            shared = block_ref[0:length, :]
            keys_ref[...] = jnp.dot(
                shared, key_ref[...], preferred_element_type=jnp.float32
            ).astype(jnp.bfloat16)
            values_ref[...] = lax.dot_general(
                value_ref[...], shared, (((1,), (1,)), ((), ())), preferred_element_type=jnp.float32
            ).astype(jnp.bfloat16)
            rows = length * ROTARY // rank
            pieces = []
            lane = lax.broadcasted_iota(jnp.int32, (rows, 2 * ROTARY), 1)
            for pair in range(rank // (2 * ROTARY)):
                tile = block_ref[length:, pair * 2 * ROTARY : (pair + 1) * 2 * ROTARY].astype(
                    jnp.float32
                )
                other = pltpu.roll(tile, ROTARY, 1)
                pieces.append(jnp.where(lane < ROTARY, tile, other))
                pieces.append(jnp.where(lane < ROTARY, other, tile))
            turned = jnp.concatenate(pieces, axis=0).astype(jnp.bfloat16)
            key_place = block * length + lax.broadcasted_iota(jnp.int32, (length, length), 0)
            visible = key_place >= starts_ref[...]
            if own:
                query_place = me * length + lax.broadcasted_iota(jnp.int32, (length, length), 1)
                visible = visible & (key_place <= query_place)
            bias_ref[...] = jnp.where(visible, 0.0, masked_score)
            for head in range(heads):
                keys = jnp.concatenate(
                    [keys_ref[:, head * CONTENT : (head + 1) * CONTENT], turned], axis=1
                )
                scores = lax.dot_general(
                    keys,
                    query_ref[head],
                    (((1,), (1,)), ((), ())),
                    preferred_element_type=jnp.float32,
                )
                scores = scores * scale + bias_ref[...]
                highest = jnp.max(scores, axis=0, keepdims=True)
                if not own:
                    before = stat_ref[head : head + 1, :]
                    highest = jnp.maximum(highest, before)
                    factor = jnp.exp2(before - highest)
                weights = jnp.exp2(scores - highest)
                total = jnp.sum(weights, axis=0, keepdims=True)
                summed = jnp.dot(
                    values_ref[head * VALUE_DIM : (head + 1) * VALUE_DIM, :],
                    weights.astype(jnp.bfloat16),
                    preferred_element_type=jnp.float32,
                )
                if not own:
                    total = total + stat_ref[heads + head : heads + head + 1, :] * factor
                    summed = summed + acc_ref[head] * factor
                stat_ref[head : head + 1, :] = highest
                stat_ref[heads + head : heads + head + 1, :] = total
                acc_ref[head] = summed

        if own:
            work()
        else:
            needed = (block >= 0) & (block <= me) & ((block + 1) * length - 1 >= first_start)
            pl.when(needed)(work)

    for place_of, block_ref in zip(places, blocks):
        process(place_of, block_ref, place_of is own_place)


def own_place(me):
    return me


def at(flip, back):
    def place(me):
        return jnp.bitwise_xor(me, flip) - back if back else jnp.bitwise_xor(me, flip)

    return place


def finish_kernel(heads, stat_ref, acc_ref, out_ref):
    for head in range(heads):
        ratio = acc_ref[head] / stat_ref[heads + head : heads + head + 1, :]
        out_ref[:, head * VALUE_DIM : (head + 1) * VALUE_DIM] = ratio.T.astype(jnp.bfloat16)


def project_kernel(rows_ref, weight_ref, out_ref):
    out_ref[...] = jnp.dot(
        rows_ref[...], weight_ref[...], preferred_element_type=jnp.float32
    ).astype(jnp.bfloat16)


def on_device(
    query_latent,
    shared_latent,
    rotary_key,
    document_start,
    query_gain,
    shared_gain,
    content_weight,
    rotary_weight,
    key_weight,
    value_weight,
    output_weight,
):
    length, rank = shared_latent.shape
    count = lax.axis_size("sp")
    groups = lax.axis_size("tp")
    heads = key_weight.shape[1] // CONTENT
    model = output_weight.shape[1]
    me = lax.axis_index("sp")
    places = (me * length + jnp.arange(length, dtype=jnp.int32)).astype(jnp.float32)
    frequency = 1.0 / rope_theta ** (jnp.arange(0, ROTARY, 2, dtype=jnp.float32) / ROTARY)
    angles = places[:, None] * frequency[None, :]
    cosine, sine = jnp.cos(angles), jnp.sin(angles)
    cos_table = jnp.concatenate([cosine] * 4, axis=1)
    sin_table = jnp.concatenate([-sine, sine] * 2, axis=1)

    packed_rows = length + length * ROTARY // rank
    mine = pl.pallas_call(
        pack_kernel,
        out_shape=jax.ShapeDtypeStruct((packed_rows, rank), jnp.bfloat16),
        in_specs=[vmem()] * 5,
        out_specs=vmem(),
        cost_estimate=pl.CostEstimate(flops=10**8, bytes_accessed=10**6, transcendentals=0),
        name="pack",
    )(shared_latent, rotary_key, shared_gain[None, :], cos_table, sin_table)

    everyone = range(count)

    def hop(value, pairs):
        return lax.ppermute(value, "sp", pairs)

    core = [(i, i ^ 1) for i in everyone]
    ahead = [(i, i + GROUP) for i in everyone if i + GROUP < count]
    ahead_again = [(i, j) for i, j in ahead if i % GROUP > 0]
    up = [(i, i ^ 2) for i in everyone if i % GROUP < 2]
    down = [(i, i ^ 2) for i in everyone if i % GROUP >= 2]
    both = [(i, i ^ 2) for i in everyone]

    back1 = hop(mine, ahead)
    side0 = hop(mine, up)
    core0 = hop(mine, core)
    back2 = hop(back1, ahead_again)
    side1 = hop(back1, both)
    core1 = hop(back1, core)
    far0 = hop(side0, core)
    side2 = hop(back2, down)
    core2 = hop(back2, core)
    far1 = hop(side1, core)
    far2 = hop(side2, core)

    queries = pl.pallas_call(
        query_kernel,
        out_shape=jax.ShapeDtypeStruct((heads, length, 2 * CONTENT), jnp.bfloat16),
        in_specs=[vmem()] * 6,
        out_specs=vmem(),
        cost_estimate=pl.CostEstimate(flops=8 * 10**8, bytes_accessed=4 * 10**6, transcendentals=0),
        name="queries",
    )(query_latent, query_gain[None, :], content_weight, rotary_weight, cos_table, sin_table)

    value_turned = value_weight.T

    def attend(state, pieces):
        stage = [place for place, _ in pieces]
        arrays = [array for _, array in pieces]
        first = state is None
        operands = [document_start, document_start[None, :], queries, key_weight, value_turned]
        operands += arrays
        aliases = {}
        if not first:
            aliases = {len(operands): 0, len(operands) + 1: 1}
            operands += list(state)
        return pl.pallas_call(
            functools.partial(attend_kernel, stage, "sp", first, False),
            out_shape=(
                jax.ShapeDtypeStruct((2 * heads, length), jnp.float32),
                jax.ShapeDtypeStruct((heads, VALUE_DIM, length), jnp.float32),
            ),
            in_specs=[smem()] + [vmem()] * (len(operands) - 1),
            out_specs=(vmem(), vmem()),
            scratch_shapes=[
                pltpu.VMEM((length, length), jnp.float32),
                pltpu.VMEM((length, heads * CONTENT), jnp.bfloat16),
                pltpu.VMEM((heads * VALUE_DIM, length), jnp.bfloat16),
            ],
            input_output_aliases=aliases,
            cost_estimate=pl.CostEstimate(
                flops=10**9 * len(pieces), bytes_accessed=5 * 10**6, transcendentals=0
            ),
            name=f"attend{len(pieces)}",
        )(*operands)

    state = attend(None, [(own_place, mine), (at(1, 0), core0)])
    state = attend(state, [(at(2, 0), side0), (at(3, 0), far0), (at(0, 4), back1), (at(1, 4), core1)])
    state = attend(state, [(at(2, 4), side1), (at(3, 4), far1), (at(1, 8), core2)])
    state = attend(state, [(at(2, 8), side2), (at(3, 8), far2)])

    attended = pl.pallas_call(
        functools.partial(finish_kernel, heads),
        out_shape=jax.ShapeDtypeStruct((length, heads * VALUE_DIM), jnp.bfloat16),
        in_specs=[vmem()] * 2,
        out_specs=vmem(),
        cost_estimate=pl.CostEstimate(flops=10**8, bytes_accessed=10**6, transcendentals=0),
        name="finish",
    )(*state)

    chunks = 8
    width = model // chunks
    pieces = []
    for chunk in range(chunks):
        term = pl.pallas_call(
            project_kernel,
            grid=(1,),
            out_shape=jax.ShapeDtypeStruct((length, width), jnp.bfloat16),
            in_specs=[
                pl.BlockSpec((length, heads * VALUE_DIM), lambda i: (0, 0)),
                pl.BlockSpec((heads * VALUE_DIM, width), lambda i, chunk=chunk: (0, chunk)),
            ],
            out_specs=pl.BlockSpec((length, width), lambda i: (0, 0)),
            cost_estimate=pl.CostEstimate(
                flops=3 * 10**8, bytes_accessed=2 * 10**6, transcendentals=0
            ),
            name=f"project{chunk}",
        )(attended, output_weight)
        total = term.astype(jnp.float32)
        for step in range(1, groups):
            pairs = [(i, (i + step) % groups) for i in range(groups)]
            total = total + lax.ppermute(term, "tp", pairs).astype(jnp.float32)
        pieces.append(total.astype(jnp.bfloat16))
    mixed = jnp.zeros((length, model), jnp.bfloat16)
    for chunk, piece in enumerate(pieces):
        mixed = lax.dynamic_update_slice(mixed, piece, (0, chunk * width))
    return mixed


def solution(mesh):
    return jax.shard_map(
        on_device,
        mesh=mesh,
        in_specs=(
            P("sp", None),
            P("sp", None),
            P("sp", None),
            P("sp"),
            P(),
            P(),
            P(None, "tp"),
            P(None, "tp"),
            P(None, "tp"),
            P(None, "tp"),
            P("tp", None),
        ),
        out_specs=P("sp", None),
        check_vma=False,
    )
```

```python
import functools

import jax
import jax.numpy as jnp
from jax import lax
from jax.experimental import pallas as pl
from jax.experimental.pallas import tpu as pltpu
from jax.sharding import PartitionSpec as P

CONTENT = 128
ROTARY = 64
VALUE_DIM = 128
GROUP = 4

norm_eps = 1e-06
rope_theta = 10000.0
masked_score = -1e30
LOG2E = 1.4426950408889634


def vmem():
    return pl.BlockSpec(memory_space=pltpu.VMEM)


def grant(mebibytes):
    return pltpu.CompilerParams(vmem_limit_bytes=mebibytes * 2**20)


def smem():
    return pl.BlockSpec(memory_space=pltpu.SMEM)


def normed(latent, gain):
    entries = latent.astype(jnp.float32)
    scale = lax.rsqrt(jnp.mean(entries * entries, axis=-1, keepdims=True) + norm_eps)
    return (entries * scale * gain).astype(jnp.bfloat16)


def swap_halves(x):
    width = x.shape[-1]
    half = ROTARY // 2
    lane = lax.broadcasted_iota(jnp.int32, x.shape, x.ndim - 1)
    ahead = pltpu.roll(x, width - half, x.ndim - 1)
    behind = pltpu.roll(x, half, x.ndim - 1)
    return jnp.where(lane % ROTARY < half, ahead, behind)


def pack_kernel(shared_ref, rotary_ref, gain_ref, cos_ref, sin_ref, out_ref):
    length, rank = shared_ref.shape
    out_ref[0:length, :] = normed(shared_ref[...], gain_ref[...])
    key = rotary_ref[...].astype(jnp.float32)
    key = jnp.concatenate([key, key], axis=-1)
    turned = key * cos_ref[...] + swap_halves(key) * sin_ref[...]
    rows = length * ROTARY // rank
    lane = lax.broadcasted_iota(jnp.int32, (rows, 2 * ROTARY), 1)
    for pair in range(rank // (2 * ROTARY)):
        low = turned[(2 * pair) * rows : (2 * pair + 1) * rows]
        high = turned[(2 * pair + 1) * rows : (2 * pair + 2) * rows]
        out_ref[length:, pair * 2 * ROTARY : (pair + 1) * 2 * ROTARY] = jnp.where(
            lane < ROTARY, low, high
        ).astype(jnp.bfloat16)


def query_kernel(latent_ref, gain_ref, content_ref, rotary_ref, cos_ref, sin_ref, out_ref):
    rows = normed(latent_ref[...], gain_ref[...])
    content = jnp.dot(rows, content_ref[...], preferred_element_type=jnp.float32)
    raw = jnp.dot(rows, rotary_ref[...], preferred_element_type=jnp.float32)
    lane = lax.broadcasted_iota(jnp.int32, (rows.shape[0], 2 * ROTARY), 1)
    for pair in range(out_ref.shape[0] // 2):
        piece = raw[:, pair * 2 * ROTARY : (pair + 1) * 2 * ROTARY]
        turned = piece * cos_ref[...] + swap_halves(piece) * sin_ref[...]
        for side in range(2):
            head = 2 * pair + side
            out_ref[head, :, 0:CONTENT] = content[
                :, head * CONTENT : (head + 1) * CONTENT
            ].astype(jnp.bfloat16)
            own = (lane < ROTARY) if side == 0 else (lane >= ROTARY)
            out_ref[head, :, CONTENT:] = jnp.where(own, turned, 0.0).astype(jnp.bfloat16)


def attend_kernel(places, axis, first, *refs):
    count = len(places)
    starts_smem, starts_ref, query_ref, key_ref, value_ref = refs[:5]
    blocks = refs[5 : 5 + count]
    refs = refs[5 + count :]
    if not first:
        old_stat, old_acc = refs[:2]
        refs = refs[2:]
    stat_ref, acc_ref, bias_ref, keys_ref, values_ref = refs
    heads = query_ref.shape[0]
    length = query_ref.shape[1]
    rank = key_ref.shape[0]
    me = lax.axis_index(axis)
    first_start = starts_smem[0]
    scale = (CONTENT + ROTARY) ** (-0.5) * LOG2E
    if not first:
        stat_ref[...] = old_stat[...]
        acc_ref[...] = old_acc[...]

    def process(place_of, block_ref, own):
        block = place_of(me)

        def work():
            shared = block_ref[0:length, :]
            keys_ref[...] = jnp.dot(
                shared, key_ref[...], preferred_element_type=jnp.float32
            ).astype(jnp.bfloat16)
            values_ref[...] = lax.dot_general(
                value_ref[...], shared, (((1,), (1,)), ((), ())), preferred_element_type=jnp.float32
            ).astype(jnp.bfloat16)
            rows = length * ROTARY // rank
            pieces = []
            lane = lax.broadcasted_iota(jnp.int32, (rows, 2 * ROTARY), 1)
            for pair in range(rank // (2 * ROTARY)):
                tile = block_ref[length:, pair * 2 * ROTARY : (pair + 1) * 2 * ROTARY].astype(
                    jnp.float32
                )
                other = pltpu.roll(tile, ROTARY, 1)
                pieces.append(jnp.where(lane < ROTARY, tile, other))
                pieces.append(jnp.where(lane < ROTARY, other, tile))
            turned = jnp.concatenate(pieces, axis=0).astype(jnp.bfloat16)
            key_place = block * length + lax.broadcasted_iota(jnp.int32, (length, length), 0)
            visible = key_place >= starts_ref[...]
            if own:
                query_place = me * length + lax.broadcasted_iota(jnp.int32, (length, length), 1)
                visible = visible & (key_place <= query_place)
            bias_ref[...] = jnp.where(visible, 0.0, masked_score)
            for head in range(heads):
                keys = jnp.concatenate(
                    [keys_ref[:, head * CONTENT : (head + 1) * CONTENT], turned], axis=1
                )
                scores = lax.dot_general(
                    keys,
                    query_ref[head],
                    (((1,), (1,)), ((), ())),
                    preferred_element_type=jnp.float32,
                )
                scores = scores * scale + bias_ref[...]
                highest = jnp.max(scores, axis=0, keepdims=True)
                if not own:
                    before = stat_ref[head : head + 1, :]
                    highest = jnp.maximum(highest, before)
                    factor = jnp.exp2(before - highest)
                weights = jnp.exp2(scores - highest)
                total = jnp.sum(weights, axis=0, keepdims=True)
                summed = jnp.dot(
                    values_ref[head * VALUE_DIM : (head + 1) * VALUE_DIM, :],
                    weights.astype(jnp.bfloat16),
                    preferred_element_type=jnp.float32,
                )
                if not own:
                    total = total + stat_ref[heads + head : heads + head + 1, :] * factor
                    summed = summed + acc_ref[head] * factor
                stat_ref[head : head + 1, :] = highest
                stat_ref[heads + head : heads + head + 1, :] = total
                acc_ref[head] = summed

        if own:
            work()
        else:
            needed = (block >= 0) & (block <= me) & ((block + 1) * length - 1 >= first_start)
            pl.when(needed)(work)

    for place_of, block_ref in zip(places, blocks):
        process(place_of, block_ref, place_of is own_place)


def own_place(me):
    return me


def at(flip, back):
    def place(me):
        return jnp.bitwise_xor(me, flip) - back if back else jnp.bitwise_xor(me, flip)

    return place


def finish_kernel(heads, stat_ref, acc_ref, out_ref):
    for head in range(heads):
        ratio = acc_ref[head] / stat_ref[heads + head : heads + head + 1, :]
        out_ref[:, head * VALUE_DIM : (head + 1) * VALUE_DIM] = ratio.T.astype(jnp.bfloat16)


def project_kernel(rows_ref, weight_ref, out_ref):
    out_ref[...] = jnp.dot(
        rows_ref[...], weight_ref[...], preferred_element_type=jnp.float32
    ).astype(jnp.bfloat16)


def on_device(
    query_latent,
    shared_latent,
    rotary_key,
    document_start,
    query_gain,
    shared_gain,
    content_weight,
    rotary_weight,
    key_weight,
    value_weight,
    output_weight,
):
    length, rank = shared_latent.shape
    count = lax.axis_size("sp")
    groups = lax.axis_size("tp")
    heads = key_weight.shape[1] // CONTENT
    model = output_weight.shape[1]
    me = lax.axis_index("sp")
    places = (me * length + jnp.arange(length, dtype=jnp.int32)).astype(jnp.float32)
    frequency = 1.0 / rope_theta ** (jnp.arange(0, ROTARY, 2, dtype=jnp.float32) / ROTARY)
    angles = places[:, None] * frequency[None, :]
    cosine, sine = jnp.cos(angles), jnp.sin(angles)
    cos_table = jnp.concatenate([cosine] * 4, axis=1)
    sin_table = jnp.concatenate([-sine, sine] * 2, axis=1)

    packed_rows = length + length * ROTARY // rank
    mine = pl.pallas_call(
        pack_kernel,
        out_shape=jax.ShapeDtypeStruct((packed_rows, rank), jnp.bfloat16),
        in_specs=[vmem()] * 5,
        out_specs=vmem(),
        cost_estimate=pl.CostEstimate(flops=10**8, bytes_accessed=10**6, transcendentals=0),
        compiler_params=grant(8),
        name="pack",
    )(shared_latent, rotary_key, shared_gain[None, :], cos_table, sin_table)

    everyone = range(count)

    def hop(value, pairs):
        return lax.ppermute(value, "sp", pairs)

    core = [(i, i ^ 1) for i in everyone]
    ahead = [(i, i + GROUP) for i in everyone if i + GROUP < count]
    ahead_again = [(i, j) for i, j in ahead if i % GROUP > 0]
    up = [(i, i ^ 2) for i in everyone if i % GROUP < 2]
    down = [(i, i ^ 2) for i in everyone if i % GROUP >= 2]
    both = [(i, i ^ 2) for i in everyone]

    back1 = hop(mine, ahead)
    side0 = hop(mine, up)
    core0 = hop(mine, core)
    back2 = hop(back1, ahead_again)
    side1 = hop(back1, both)
    core1 = hop(back1, core)
    far0 = hop(side0, core)
    side2 = hop(back2, down)
    core2 = hop(back2, core)
    far1 = hop(side1, core)
    far2 = hop(side2, core)

    queries = pl.pallas_call(
        query_kernel,
        out_shape=jax.ShapeDtypeStruct((heads, length, 2 * CONTENT), jnp.bfloat16),
        in_specs=[vmem()] * 6,
        out_specs=vmem(),
        cost_estimate=pl.CostEstimate(flops=8 * 10**8, bytes_accessed=4 * 10**6, transcendentals=0),
        compiler_params=grant(16),
        name="queries",
    )(query_latent, query_gain[None, :], content_weight, rotary_weight, cos_table, sin_table)

    value_turned = value_weight.T

    def attend(state, pieces):
        stage = [place for place, _ in pieces]
        arrays = [array for _, array in pieces]
        first = state is None
        operands = [document_start, document_start[None, :], queries, key_weight, value_turned]
        operands += arrays
        aliases = {}
        if not first:
            aliases = {len(operands): 0, len(operands) + 1: 1}
            operands += list(state)
        return pl.pallas_call(
            functools.partial(attend_kernel, stage, "sp", first),
            out_shape=(
                jax.ShapeDtypeStruct((2 * heads, length), jnp.float32),
                jax.ShapeDtypeStruct((heads, VALUE_DIM, length), jnp.float32),
            ),
            in_specs=[smem()] + [vmem()] * (len(operands) - 1),
            out_specs=(vmem(), vmem()),
            scratch_shapes=[
                pltpu.VMEM((length, length), jnp.float32),
                pltpu.VMEM((length, heads * CONTENT), jnp.bfloat16),
                pltpu.VMEM((heads * VALUE_DIM, length), jnp.bfloat16),
            ],
            input_output_aliases=aliases,
            cost_estimate=pl.CostEstimate(
                flops=10**9 * len(pieces), bytes_accessed=5 * 10**6, transcendentals=0
            ),
            compiler_params=grant(24),
        )(*operands)

    state = attend(None, [(own_place, mine), (at(1, 0), core0)])
    state = attend(state, [(at(2, 0), side0), (at(0, 4), back1)])
    state = attend(state, [(at(3, 0), far0), (at(1, 4), core1), (at(2, 4), side1)])
    state = attend(state, [(at(3, 4), far1), (at(1, 8), core2)])
    state = attend(state, [(at(2, 8), side2), (at(3, 8), far2)])

    attended = pl.pallas_call(
        functools.partial(finish_kernel, heads),
        out_shape=jax.ShapeDtypeStruct((length, heads * VALUE_DIM), jnp.bfloat16),
        in_specs=[vmem()] * 2,
        out_specs=vmem(),
        cost_estimate=pl.CostEstimate(flops=10**8, bytes_accessed=10**6, transcendentals=0),
        compiler_params=grant(8),
        name="finish",
    )(*state)

    chunks = 8
    width = model // chunks
    pieces = []
    for chunk in range(chunks):
        term = pl.pallas_call(
            project_kernel,
            grid=(1,),
            out_shape=jax.ShapeDtypeStruct((length, width), jnp.bfloat16),
            in_specs=[
                pl.BlockSpec((length, heads * VALUE_DIM), lambda i: (0, 0)),
                pl.BlockSpec((heads * VALUE_DIM, width), lambda i, chunk=chunk: (0, chunk)),
            ],
            out_specs=pl.BlockSpec((length, width), lambda i: (0, 0)),
            cost_estimate=pl.CostEstimate(
                flops=3 * 10**8, bytes_accessed=2 * 10**6, transcendentals=0
            ),
            compiler_params=grant(8),
        )(attended, output_weight)
        total = term.astype(jnp.float32)
        for step in range(1, groups):
            pairs = [(i, (i + step) % groups) for i in range(groups)]
            total = total + lax.ppermute(term, "tp", pairs).astype(jnp.float32)
        pieces.append(total.astype(jnp.bfloat16))
    mixed = jnp.zeros((length, model), jnp.bfloat16)
    for chunk, piece in enumerate(pieces):
        mixed = lax.dynamic_update_slice(mixed, piece, (0, chunk * width))
    return mixed


def solution(mesh):
    return jax.shard_map(
        on_device,
        mesh=mesh,
        in_specs=(
            P("sp", None),
            P("sp", None),
            P("sp", None),
            P("sp"),
            P(),
            P(),
            P(None, "tp"),
            P(None, "tp"),
            P(None, "tp"),
            P(None, "tp"),
            P("tp", None),
        ),
        out_specs=P("sp", None),
        check_vma=False,
    )
```

```python
import functools

import jax
import jax.numpy as jnp
from jax import lax
from jax.experimental import pallas as pl
from jax.experimental.pallas import tpu as pltpu
from jax.sharding import PartitionSpec as P

CONTENT = 128
ROTARY = 64
VALUE_DIM = 128
GROUP = 4
KINDS = ("quad", "pair", "pair")

norm_eps = 1e-06
rope_theta = 10000.0
masked_score = -1e30
LOG2E = 1.4426950408889634


def vmem():
    return pl.BlockSpec(memory_space=pltpu.VMEM)


def grant(mebibytes):
    return pltpu.CompilerParams(vmem_limit_bytes=mebibytes * 2**20)


def hbm():
    return pl.BlockSpec(memory_space=pltpu.HBM)


def smem():
    return pl.BlockSpec(memory_space=pltpu.SMEM)


def normed(latent, gain):
    entries = latent.astype(jnp.float32)
    scale = lax.rsqrt(jnp.mean(entries * entries, axis=-1, keepdims=True) + norm_eps)
    return (entries * scale * gain).astype(jnp.bfloat16)


def swap_halves(x):
    width = x.shape[-1]
    half = ROTARY // 2
    lane = lax.broadcasted_iota(jnp.int32, x.shape, x.ndim - 1)
    ahead = pltpu.roll(x, width - half, x.ndim - 1)
    behind = pltpu.roll(x, half, x.ndim - 1)
    return jnp.where(lane % ROTARY < half, ahead, behind)


def load(pairs, sems):
    copies = [pltpu.make_async_copy(src, dst, sems.at[k]) for k, (src, dst) in enumerate(pairs)]
    for copy in copies:
        copy.start()
    return copies


def pack_kernel(cuts, axis, shared_hbm, rotary_hbm, gain_hbm, weight_hbm, cos_ref, sin_ref, *refs):
    out_ref, parts, refs = refs[0], refs[1 : 1 + len(cuts)], refs[1 + len(cuts) :]
    shared_ref, rotary_ref, gain_ref, sems = refs
    length, rank = shared_ref.shape
    half = ROTARY // 2
    me = lax.axis_index(axis)
    pairs = [(rotary_hbm, rotary_ref), (gain_hbm, gain_ref), (shared_hbm, shared_ref)]
    for (base, size, kind), part_ref in zip(cuts, parts):
        start = pl.multiple_of(base + slot_of(me, kind) * size, 128)
        pairs.append((weight_hbm.at[:, pl.ds(start, size)], part_ref))
    copies = load(pairs, sems)
    copies[0].wait()
    key = rotary_ref[...].astype(jnp.float32)
    low, high = key[:half], key[half:]
    cosine, sine = cos_ref[...], sin_ref[...]
    turned = jnp.concatenate([low * cosine - high * sine, low * sine + high * cosine], axis=0)
    turned = jnp.concatenate([turned, turned], axis=0).T
    rows = length * ROTARY // rank
    lane = lax.broadcasted_iota(jnp.int32, (rows, 2 * ROTARY), 1)
    for pair in range(rank // (2 * ROTARY)):
        low = turned[(2 * pair) * rows : (2 * pair + 1) * rows]
        high = turned[(2 * pair + 1) * rows : (2 * pair + 2) * rows]
        out_ref[length:, pair * 2 * ROTARY : (pair + 1) * 2 * ROTARY] = jnp.where(
            lane < ROTARY, low, high
        ).astype(jnp.bfloat16)
    copies[1].wait()
    copies[2].wait()
    out_ref[0:length, :] = normed(shared_ref[...], gain_ref[...])
    for copy in copies[3:]:
        copy.wait()


def begin_kernel(axis, *refs):
    hbm, refs = refs[:6], refs[6:]
    starts_ref, block_ref, cos_ref, sin_ref = refs[:4]
    query_ref, turned_value_ref, stat_ref, acc_ref = refs[4:8]
    held, refs = refs[8:14], refs[14:]
    scratch, sems = refs[:-1], refs[-1]
    copies = load(list(zip(hbm, held)), sems)
    latent_ref, gain_ref, content_ref, rotary_ref, value_ref, key_ref = held
    cos4 = jnp.concatenate([cos_ref[...]] * 4, axis=0).T
    sin4 = jnp.concatenate([-sin_ref[...], sin_ref[...]] * 2, axis=0).T
    copies[0].wait()
    copies[1].wait()
    rows = normed(latent_ref[...], gain_ref[...])
    copies[2].wait()
    content = jnp.dot(rows, content_ref[...], preferred_element_type=jnp.float32)
    for head in range(query_ref.shape[0]):
        query_ref[head, :, 0:CONTENT] = content[:, head * CONTENT : (head + 1) * CONTENT].astype(
            jnp.bfloat16
        )
    copies[3].wait()
    raw = jnp.dot(rows, rotary_ref[...], preferred_element_type=jnp.float32)
    lane = lax.broadcasted_iota(jnp.int32, (rows.shape[0], 2 * ROTARY), 1)
    for pair in range(query_ref.shape[0] // 2):
        piece = raw[:, pair * 2 * ROTARY : (pair + 1) * 2 * ROTARY]
        turned = piece * cos4 + swap_halves(piece) * sin4
        for side in range(2):
            own = (lane < ROTARY) if side == 0 else (lane >= ROTARY)
            query_ref[2 * pair + side, :, CONTENT:] = jnp.where(own, turned, 0.0).astype(
                jnp.bfloat16
            )
    copies[4].wait()
    turned_value_ref[...] = value_ref[...].T
    copies[5].wait()
    me = lax.axis_index(axis)
    absorb(
        me, me, True, block_ref, starts_ref, query_ref, key_ref, turned_value_ref, stat_ref, acc_ref, *scratch
    )


def absorb(
    me, block, own, block_ref, starts_ref, query_ref, key_ref, value_ref, stat_ref, acc_ref,
    bias_ref, keys_ref, values_ref, scores_ref, weights_ref,
):
    heads, length = query_ref.shape[0], query_ref.shape[1]
    rank = key_ref.shape[0]
    scale = (CONTENT + ROTARY) ** (-0.5) * LOG2E
    shared = block_ref[0:length, :]
    keys_ref[...] = jnp.dot(shared, key_ref[...], preferred_element_type=jnp.float32).astype(
        jnp.bfloat16
    )
    values_ref[...] = lax.dot_general(
        value_ref[...], shared, (((1,), (1,)), ((), ())), preferred_element_type=jnp.float32
    ).astype(jnp.bfloat16)
    rows = length * ROTARY // rank
    pieces = []
    lane = lax.broadcasted_iota(jnp.int32, (rows, 2 * ROTARY), 1)
    for pair in range(rank // (2 * ROTARY)):
        tile = block_ref[length:, pair * 2 * ROTARY : (pair + 1) * 2 * ROTARY].astype(jnp.float32)
        other = pltpu.roll(tile, ROTARY, 1)
        pieces.append(jnp.where(lane < ROTARY, tile, other))
        pieces.append(jnp.where(lane < ROTARY, other, tile))
    turned = jnp.concatenate(pieces, axis=0).astype(jnp.bfloat16)
    key_place = block * length + lax.broadcasted_iota(jnp.int32, (length, length), 0)
    visible = key_place >= starts_ref[...]
    if own:
        query_place = me * length + lax.broadcasted_iota(jnp.int32, (length, length), 1)
        visible = visible & (key_place <= query_place)
    bias_ref[...] = jnp.where(visible, 0.0, masked_score)
    tops, factors = [], []
    for head in range(heads):
        keys = jnp.concatenate([keys_ref[:, head * CONTENT : (head + 1) * CONTENT], turned], axis=1)
        scores = lax.dot_general(
            keys, query_ref[head], (((1,), (1,)), ((), ())), preferred_element_type=jnp.float32
        )
        scores = scores * scale + bias_ref[...]
        scores_ref[head] = scores
        highest = jnp.max(scores, axis=0, keepdims=True)
        if not own:
            highest = jnp.maximum(highest, stat_ref[head : head + 1, :])
        tops.append(highest)
    piece = 64
    for head in range(heads):
        total = jnp.zeros((1, length), jnp.float32)
        for row in range(0, length, piece):
            weights = jnp.exp2(scores_ref[head, row : row + piece, :] - tops[head])
            total = total + jnp.sum(weights, axis=0, keepdims=True)
            weights_ref[head, row : row + piece, :] = weights.astype(jnp.bfloat16)
        if not own:
            factor = jnp.exp2(stat_ref[head : head + 1, :] - tops[head])
            factors.append(factor)
            total = total + stat_ref[heads + head : heads + head + 1, :] * factor
        stat_ref[head : head + 1, :] = tops[head]
        stat_ref[heads + head : heads + head + 1, :] = total
    for head in range(heads):
        summed = jnp.dot(
            values_ref[head * VALUE_DIM : (head + 1) * VALUE_DIM, :],
            weights_ref[head],
            preferred_element_type=jnp.float32,
        )
        acc_ref[head] = summed if own else acc_ref[head] * factors[head] + summed


def work_area(heads, length):
    return [
        pltpu.VMEM((length, length), jnp.float32),
        pltpu.VMEM((length, heads * CONTENT), jnp.bfloat16),
        pltpu.VMEM((heads * VALUE_DIM, length), jnp.bfloat16),
        pltpu.VMEM((heads, length, length), jnp.float32),
        pltpu.VMEM((heads, length, length), jnp.bfloat16),
    ]


def attend_kernel(places, axis, *refs):
    count = len(places)
    starts_smem, starts_ref, query_ref, key_ref, value_ref = refs[:5]
    blocks, refs = refs[5 : 5 + count], refs[5 + count :]
    old_stat, old_acc, stat_ref, acc_ref = refs[:4]
    scratch = refs[4:]
    length = query_ref.shape[1]
    me = lax.axis_index(axis)
    stat_ref[...] = old_stat[...]
    acc_ref[...] = old_acc[...]
    for place_of, block_ref in zip(places, blocks):
        block = place_of(me)
        needed = (block >= 0) & (block <= me) & ((block + 1) * length - 1 >= starts_smem[0])
        pl.when(needed)(
            functools.partial(
                absorb, me, block, False, block_ref, starts_ref, query_ref, key_ref, value_ref,
                stat_ref, acc_ref, *scratch,
            )
        )


def at(flip, back):
    def place(me):
        return jnp.bitwise_xor(me, flip) - back if back else jnp.bitwise_xor(me, flip)

    return place


def finish_kernel(heads, stat_ref, acc_ref, out_ref):
    for head in range(heads):
        ratio = acc_ref[head] / stat_ref[heads + head : heads + head + 1, :]
        out_ref[:, head * VALUE_DIM : (head + 1) * VALUE_DIM] = ratio.T.astype(jnp.bfloat16)


def project_kernel(rows_ref, weight_ref, out_ref):
    tile = 512

    @pl.loop(0, weight_ref.shape[1] // tile)
    def _(step):
        columns = pl.ds(pl.multiple_of(step * tile, tile), tile)
        out_ref[:, columns] = jnp.dot(
            rows_ref[...], weight_ref[:, columns], preferred_element_type=jnp.float32
        ).astype(jnp.bfloat16)


def slot_of(me, kind):
    if kind == "quad":
        return jnp.bitwise_and(me, 7)
    return jnp.bitwise_and(lax.shift_right_logical(me, 2), 1) * 2 + jnp.bitwise_and(me, 1)


def combine_kernel(places, axis, rows_ref, ours_ref, *refs):
    me = lax.axis_index(axis)
    count = len(places)
    pieces, out_hbm, refs = refs[:count], refs[count], refs[count + 1 :]
    held_ref, done_ref, sems, out_sems = refs
    copies = []
    for k, (base, size, kind, change) in enumerate(places):
        start = base + jnp.bitwise_xor(slot_of(me, kind), change) * size
        columns = pl.ds(pl.multiple_of(start, 128), size)
        copies.append(pltpu.make_async_copy(pieces[k], held_ref.at[:, columns], sems.at[k]))
    ahead = 6
    for copy in copies[:ahead]:
        copy.start()
    leaving = []
    for k in range(0, count, 2):
        base, size, kind, change = places[k]
        start = base + (jnp.bitwise_xor(slot_of(me, kind), change) // 2) * (2 * size)
        columns = pl.ds(pl.multiple_of(start, 256), 2 * size)
        for late in (k, k + 1):
            copies[late].wait()
            if late + ahead < count:
                copies[late + ahead].start()
        term = jnp.dot(rows_ref[...], held_ref[:, columns], preferred_element_type=jnp.float32)
        term = term.astype(jnp.bfloat16).astype(jnp.float32)
        done_ref[:, columns] = (ours_ref[:, columns].astype(jnp.float32) + term).astype(
            jnp.bfloat16
        )
        out = pltpu.make_async_copy(
            done_ref.at[:, columns], out_hbm.at[:, columns], out_sems.at[k // 2]
        )
        out.start()
        leaving.append(out)
    for out in leaving:
        out.wait()


def on_device(
    query_latent,
    shared_latent,
    rotary_key,
    document_start,
    query_gain,
    shared_gain,
    content_weight,
    rotary_weight,
    key_weight,
    value_weight,
    output_weight,
):
    length, rank = shared_latent.shape
    count = lax.axis_size("sp")
    groups = lax.axis_size("tp")
    heads = key_weight.shape[1] // CONTENT
    model = output_weight.shape[1]
    me = lax.axis_index("sp")
    position = (me * length + jnp.arange(length, dtype=jnp.int32)).astype(jnp.float32)
    frequency = 1.0 / rope_theta ** (jnp.arange(0, ROTARY, 2, dtype=jnp.float32) / ROTARY)
    angles = frequency[:, None] * position[None, :]
    cosine, sine = jnp.cos(angles), jnp.sin(angles)

    plan = groups == 2 and count % 8 == 0 and model % 2048 == 0
    swap = [(0, 1), (1, 0)]
    size = model // 16
    cuts, base = [], 0
    for kind in KINDS if plan else ():
        cuts.append((base, size, kind))
        base += size * (8 if kind == "quad" else 4)

    packed_rows = length + length * ROTARY // rank
    mine, *parts = pl.pallas_call(
        functools.partial(pack_kernel, cuts, "sp"),
        out_shape=[jax.ShapeDtypeStruct((packed_rows, rank), jnp.bfloat16)]
        + [jax.ShapeDtypeStruct((output_weight.shape[0], size), jnp.bfloat16) for _ in cuts],
        in_specs=[hbm()] * 4 + [vmem()] * 2,
        out_specs=[vmem()] * (1 + len(cuts)),
        scratch_shapes=[
            pltpu.VMEM((length, rank), jnp.bfloat16),
            pltpu.VMEM((ROTARY, length), jnp.bfloat16),
            pltpu.VMEM((1, rank), jnp.float32),
            pltpu.SemaphoreType.DMA((3 + len(cuts),)),
        ],
        cost_estimate=pl.CostEstimate(flops=10**8, bytes_accessed=10**6, transcendentals=0),
        compiler_params=grant(60),
        name="pack",
    )(shared_latent, rotary_key.T, shared_gain[None, :], output_weight, cosine, sine)

    everyone = range(count)

    def hop(value, pairs):
        return lax.ppermute(value, "sp", pairs)

    core = [(i, i ^ 1) for i in everyone]
    ahead = [(i, i + GROUP) for i in everyone if i + GROUP < count]
    ahead_again = [(i, j) for i, j in ahead if i % GROUP > 0]
    up = [(i, i ^ 2) for i in everyone if i % GROUP < 2]
    down = [(i, i ^ 2) for i in everyone if i % GROUP >= 2]
    both = [(i, i ^ 2) for i in everyone]

    back1 = hop(mine, ahead)
    side0 = hop(mine, up)
    core0 = hop(mine, core)
    back2 = hop(back1, ahead_again)
    side1 = hop(back1, both)
    core1 = hop(back1, core)
    far0 = hop(side0, core)
    side2 = hop(back2, down)
    core2 = hop(back2, core)
    far1 = hop(side1, core)
    far2 = hop(side2, core)

    places, pieces = [], []
    if plan:
        over_z = [(i, i ^ 4) for i in everyone]
        over_y = [(i, i ^ 2) for i in everyone]
        for chunk, (base, size, kind) in enumerate(cuts):
            pulled = lax.ppermute(parts[chunk], "tp", swap)
            crossed = hop(pulled, over_z)
            if kind == "quad":
                arrived = [(0, pulled), (4, crossed)]
                arrived += [(2, hop(pulled, over_y)), (6, hop(crossed, over_y))]
            else:
                arrived = [(0, pulled), (2, crossed)]
            for change, piece in arrived:
                places.append((base, size, kind, change))
                pieces.append(piece)
                places.append((base, size, kind, change + 1))
                pieces.append(hop(piece, core))

    latents = (query_latent, query_gain[None, :], content_weight, rotary_weight, value_weight, key_weight)
    queries, value_turned, stat, acc = pl.pallas_call(
        functools.partial(begin_kernel, "sp"),
        out_shape=(
            jax.ShapeDtypeStruct((heads, length, 2 * CONTENT), jnp.bfloat16),
            jax.ShapeDtypeStruct((heads * VALUE_DIM, rank), jnp.bfloat16),
            jax.ShapeDtypeStruct((2 * heads, length), jnp.float32),
            jax.ShapeDtypeStruct((heads, VALUE_DIM, length), jnp.float32),
        ),
        in_specs=[hbm()] * 6 + [vmem()] * 4,
        out_specs=(vmem(),) * 4,
        scratch_shapes=[pltpu.VMEM(x.shape, x.dtype) for x in latents]
        + work_area(heads, length)
        + [pltpu.SemaphoreType.DMA((6,))],
        cost_estimate=pl.CostEstimate(flops=2 * 10**9, bytes_accessed=6 * 10**6, transcendentals=0),
        compiler_params=grant(58),
        name="begin",
    )(*latents, document_start[None, :], mine, cosine, sine)
    state = (stat, acc)

    def attend(state, pieces):
        stage = [place for place, _ in pieces]
        operands = [document_start, document_start[None, :], queries, key_weight, value_turned]
        operands += [array for _, array in pieces]
        aliases = {len(operands): 0, len(operands) + 1: 1}
        operands += list(state)
        return pl.pallas_call(
            functools.partial(attend_kernel, stage, "sp"),
            out_shape=(
                jax.ShapeDtypeStruct((2 * heads, length), jnp.float32),
                jax.ShapeDtypeStruct((heads, VALUE_DIM, length), jnp.float32),
            ),
            in_specs=[smem()] + [vmem()] * (len(operands) - 1),
            out_specs=(vmem(), vmem()),
            scratch_shapes=work_area(heads, length),
            input_output_aliases=aliases,
            cost_estimate=pl.CostEstimate(
                flops=10**9 * len(stage), bytes_accessed=5 * 10**6, transcendentals=0
            ),
            compiler_params=grant(18),
        )(*operands)

    state = attend(state, [(at(1, 0), core0), (at(2, 0), side0), (at(0, 4), back1)])
    state = attend(state, [(at(3, 0), far0), (at(1, 4), core1), (at(2, 4), side1)])
    state = attend(state, [(at(3, 4), far1), (at(1, 8), core2)])
    state = attend(state, [(at(2, 8), side2), (at(3, 8), far2)])

    attended = pl.pallas_call(
        functools.partial(finish_kernel, heads),
        out_shape=jax.ShapeDtypeStruct((length, heads * VALUE_DIM), jnp.bfloat16),
        in_specs=[vmem()] * 2,
        out_specs=vmem(),
        cost_estimate=pl.CostEstimate(flops=10**8, bytes_accessed=10**6, transcendentals=0),
        compiler_params=grant(8),
        name="finish",
    )(*state)

    if not plan:
        mixed = jnp.dot(attended, output_weight, preferred_element_type=jnp.float32)
        return lax.psum(mixed.astype(jnp.bfloat16), "tp")

    theirs = lax.ppermute(attended, "tp", swap)
    ours = pl.pallas_call(
        project_kernel,
        out_shape=jax.ShapeDtypeStruct((length, model), jnp.bfloat16),
        in_specs=[vmem()] * 2,
        out_specs=vmem(),
        cost_estimate=pl.CostEstimate(
            flops=2 * 10**9, bytes_accessed=10**7, transcendentals=0
        ),
        compiler_params=grant(14),
        name="ours",
    )(attended, output_weight)
    mixed = pl.pallas_call(
        functools.partial(combine_kernel, places, "sp"),
        out_shape=jax.ShapeDtypeStruct((length, model), jnp.bfloat16),
        in_specs=[vmem()] * 2 + [hbm()] * len(pieces),
        out_specs=hbm(),
        scratch_shapes=[
            pltpu.VMEM(output_weight.shape, jnp.bfloat16),
            pltpu.VMEM((length, model), jnp.bfloat16),
            pltpu.SemaphoreType.DMA((len(pieces),)),
            pltpu.SemaphoreType.DMA((len(pieces) // 2,)),
        ],
        cost_estimate=pl.CostEstimate(
            flops=2 * 10**9, bytes_accessed=10**7, transcendentals=0
        ),
        compiler_params=grant(20),
        name="theirs",
    )(theirs, ours, *pieces)
    return mixed


def solution(mesh):
    return jax.shard_map(
        on_device,
        mesh=mesh,
        in_specs=(
            P("sp", None),
            P("sp", None),
            P("sp", None),
            P("sp"),
            P(),
            P(),
            P(None, "tp"),
            P(None, "tp"),
            P(None, "tp"),
            P(None, "tp"),
            P("tp", None),
        ),
        out_specs=P("sp", None),
        check_vma=False,
    )
```

```python
import functools

import jax
import jax.numpy as jnp
from jax import lax
from jax.experimental import pallas as pl
from jax.experimental.pallas import tpu as pltpu
from jax.sharding import PartitionSpec as P

CONTENT = 128
ROTARY = 64
VALUE_DIM = 128
GROUP = 4
KINDS = (("quad", 1), ("z", 2), ("y", 2), ("z", 2))
EARLY = 16

norm_eps = 1e-06
rope_theta = 10000.0
masked_score = -1e30
LOG2E = 1.4426950408889634


def vmem():
    return pl.BlockSpec(memory_space=pltpu.VMEM)


def grant(mebibytes):
    return pltpu.CompilerParams(vmem_limit_bytes=mebibytes * 2**20)


def hbm():
    return pl.BlockSpec(memory_space=pltpu.HBM)


def smem():
    return pl.BlockSpec(memory_space=pltpu.SMEM)


def normed(latent, gain):
    entries = latent.astype(jnp.float32)
    scale = lax.rsqrt(jnp.mean(entries * entries, axis=-1, keepdims=True) + norm_eps)
    return (entries * scale * gain).astype(jnp.bfloat16)


def swap_halves(x):
    width = x.shape[-1]
    half = ROTARY // 2
    lane = lax.broadcasted_iota(jnp.int32, x.shape, x.ndim - 1)
    ahead = pltpu.roll(x, width - half, x.ndim - 1)
    behind = pltpu.roll(x, half, x.ndim - 1)
    return jnp.where(lane % ROTARY < half, ahead, behind)


def load(pairs, sems):
    copies = [pltpu.make_async_copy(src, dst, sems.at[k]) for k, (src, dst) in enumerate(pairs)]
    for copy in copies:
        copy.start()
    return copies


def cut_kernel(cuts, axis, weight_hbm, *refs):
    parts, sems = refs[:-1], refs[-1]
    me = lax.axis_index(axis)
    pairs = []
    for (base, size, kind), part_ref in zip(cuts, parts):
        start = pl.multiple_of(base + slot_of(me, kind) * size, 128)
        pairs.append((weight_hbm.at[:, pl.ds(start, size)], part_ref))
    for copy in load(pairs, sems):
        copy.wait()


def pack_kernel(shared_ref, rotary_ref, gain_ref, cos_ref, sin_ref, out_ref):
    length, rank = shared_ref.shape
    half = ROTARY // 2
    key = rotary_ref[...].astype(jnp.float32)
    low, high = key[:half], key[half:]
    cosine, sine = cos_ref[...], sin_ref[...]
    turned = jnp.concatenate([low * cosine - high * sine, low * sine + high * cosine], axis=0)
    turned = jnp.concatenate([turned, turned], axis=0).T
    rows = length * ROTARY // rank
    lane = lax.broadcasted_iota(jnp.int32, (rows, 2 * ROTARY), 1)
    for pair in range(rank // (2 * ROTARY)):
        low = turned[(2 * pair) * rows : (2 * pair + 1) * rows]
        high = turned[(2 * pair + 1) * rows : (2 * pair + 2) * rows]
        out_ref[length:, pair * 2 * ROTARY : (pair + 1) * 2 * ROTARY] = jnp.where(
            lane < ROTARY, low, high
        ).astype(jnp.bfloat16)
    out_ref[0:length, :] = normed(shared_ref[...], gain_ref[...])


def begin_kernel(axis, *refs):
    latent_ref, gain_ref, content_ref, rotary_ref, value_ref, key_ref = refs[:6]
    starts_ref, block_ref, cos_ref, sin_ref = refs[6:10]
    query_ref, turned_value_ref, stat_ref, acc_ref = refs[10:14]
    scratch = refs[14:]
    cos4 = jnp.concatenate([cos_ref[...]] * 4, axis=0).T
    sin4 = jnp.concatenate([-sin_ref[...], sin_ref[...]] * 2, axis=0).T
    rows = normed(latent_ref[...], gain_ref[...])
    content = jnp.dot(rows, content_ref[...], preferred_element_type=jnp.float32)
    for head in range(query_ref.shape[0]):
        query_ref[head, :, 0:CONTENT] = content[:, head * CONTENT : (head + 1) * CONTENT].astype(
            jnp.bfloat16
        )
    raw = jnp.dot(rows, rotary_ref[...], preferred_element_type=jnp.float32)
    lane = lax.broadcasted_iota(jnp.int32, (rows.shape[0], 2 * ROTARY), 1)
    for pair in range(query_ref.shape[0] // 2):
        piece = raw[:, pair * 2 * ROTARY : (pair + 1) * 2 * ROTARY]
        turned = piece * cos4 + swap_halves(piece) * sin4
        for side in range(2):
            own = (lane < ROTARY) if side == 0 else (lane >= ROTARY)
            query_ref[2 * pair + side, :, CONTENT:] = jnp.where(own, turned, 0.0).astype(
                jnp.bfloat16
            )
    turned_value_ref[...] = value_ref[...].T
    me = lax.axis_index(axis)
    absorb(
        me, me, True, block_ref, starts_ref, query_ref, key_ref, turned_value_ref, stat_ref, acc_ref, *scratch
    )


def absorb(
    me, block, own, block_ref, starts_ref, query_ref, key_ref, value_ref, stat_ref, acc_ref,
    bias_ref, keys_ref, values_ref, scores_ref, weights_ref,
):
    heads, length = query_ref.shape[0], query_ref.shape[1]
    rank = key_ref.shape[0]
    scale = (CONTENT + ROTARY) ** (-0.5) * LOG2E
    shared = block_ref[0:length, :]
    keys_ref[...] = jnp.dot(shared, key_ref[...], preferred_element_type=jnp.float32).astype(
        jnp.bfloat16
    )
    values_ref[...] = lax.dot_general(
        value_ref[...], shared, (((1,), (1,)), ((), ())), preferred_element_type=jnp.float32
    ).astype(jnp.bfloat16)
    rows = length * ROTARY // rank
    pieces = []
    lane = lax.broadcasted_iota(jnp.int32, (rows, 2 * ROTARY), 1)
    for pair in range(rank // (2 * ROTARY)):
        tile = block_ref[length:, pair * 2 * ROTARY : (pair + 1) * 2 * ROTARY].astype(jnp.float32)
        other = pltpu.roll(tile, ROTARY, 1)
        pieces.append(jnp.where(lane < ROTARY, tile, other))
        pieces.append(jnp.where(lane < ROTARY, other, tile))
    turned = jnp.concatenate(pieces, axis=0).astype(jnp.bfloat16)
    key_place = block * length + lax.broadcasted_iota(jnp.int32, (length, length), 0)
    visible = key_place >= starts_ref[...]
    if own:
        query_place = me * length + lax.broadcasted_iota(jnp.int32, (length, length), 1)
        visible = visible & (key_place <= query_place)
    bias_ref[...] = jnp.where(visible, 0.0, masked_score)
    tops, factors = [], []
    for head in range(heads):
        keys = jnp.concatenate([keys_ref[:, head * CONTENT : (head + 1) * CONTENT], turned], axis=1)
        scores = lax.dot_general(
            keys, query_ref[head], (((1,), (1,)), ((), ())), preferred_element_type=jnp.float32
        )
        scores = scores * scale + bias_ref[...]
        scores_ref[head] = scores
        highest = jnp.max(scores, axis=0, keepdims=True)
        if not own:
            highest = jnp.maximum(highest, stat_ref[head : head + 1, :])
        tops.append(highest)
    piece = 64
    for head in range(heads):
        total = jnp.zeros((1, length), jnp.float32)
        for row in range(0, length, piece):
            weights = jnp.exp2(scores_ref[head, row : row + piece, :] - tops[head])
            total = total + jnp.sum(weights, axis=0, keepdims=True)
            weights_ref[head, row : row + piece, :] = weights.astype(jnp.bfloat16)
        if not own:
            factor = jnp.exp2(stat_ref[head : head + 1, :] - tops[head])
            factors.append(factor)
            total = total + stat_ref[heads + head : heads + head + 1, :] * factor
        stat_ref[head : head + 1, :] = tops[head]
        stat_ref[heads + head : heads + head + 1, :] = total
    for head in range(heads):
        summed = jnp.dot(
            values_ref[head * VALUE_DIM : (head + 1) * VALUE_DIM, :],
            weights_ref[head],
            preferred_element_type=jnp.float32,
        )
        acc_ref[head] = summed if own else acc_ref[head] * factors[head] + summed


def work_area(heads, length):
    return [
        pltpu.VMEM((length, length), jnp.float32),
        pltpu.VMEM((length, heads * CONTENT), jnp.bfloat16),
        pltpu.VMEM((heads * VALUE_DIM, length), jnp.bfloat16),
        pltpu.VMEM((heads, length, length), jnp.float32),
        pltpu.VMEM((heads, length, length), jnp.bfloat16),
    ]


def attend_kernel(places, axis, *refs):
    count = len(places)
    starts_smem, starts_ref, query_ref, key_ref, value_ref = refs[:5]
    blocks, refs = refs[5 : 5 + count], refs[5 + count :]
    old_stat, old_acc, stat_ref, acc_ref = refs[:4]
    scratch = refs[4:]
    length = query_ref.shape[1]
    me = lax.axis_index(axis)
    stat_ref[...] = old_stat[...]
    acc_ref[...] = old_acc[...]
    for place_of, block_ref in zip(places, blocks):
        block = place_of(me)
        needed = (block >= 0) & (block <= me) & ((block + 1) * length - 1 >= starts_smem[0])
        pl.when(needed)(
            functools.partial(
                absorb, me, block, False, block_ref, starts_ref, query_ref, key_ref, value_ref,
                stat_ref, acc_ref, *scratch,
            )
        )


def at(flip, back):
    def place(me):
        return jnp.bitwise_xor(me, flip) - back if back else jnp.bitwise_xor(me, flip)

    return place


def finish_kernel(heads, stat_ref, acc_ref, out_ref):
    for head in range(heads):
        ratio = acc_ref[head] / stat_ref[heads + head : heads + head + 1, :]
        out_ref[:, head * VALUE_DIM : (head + 1) * VALUE_DIM] = ratio.T.astype(jnp.bfloat16)


def project_kernel(rows_ref, weight_ref, out_ref):
    tile = 512

    @pl.loop(0, weight_ref.shape[1] // tile)
    def _(step):
        columns = pl.ds(pl.multiple_of(step * tile, tile), tile)
        out_ref[:, columns] = jnp.dot(
            rows_ref[...], weight_ref[:, columns], preferred_element_type=jnp.float32
        ).astype(jnp.bfloat16)


def slot_of(me, kind):
    if kind == "quad":
        return jnp.bitwise_and(me, 7)
    bit = 2 if kind == "z" else 1
    return jnp.bitwise_and(lax.shift_right_logical(me, bit), 1) * 2 + jnp.bitwise_and(me, 1)


def combine_kernel(places, axis, rows_ref, ours_ref, *refs):
    me = lax.axis_index(axis)
    count = len(places)
    pieces, (out_hbm, done_ref, out_sems) = refs[:count], refs[-3:]
    rows = rows_ref[...]
    leaving = []
    for k in range(0, count, 2):
        base, size, kind, change = places[k]
        starts = [
            pl.multiple_of(base + jnp.bitwise_xor(slot_of(me, kind), flip) * size, 128)
            for flip in (change, change + 1)
        ]
        if size % 256 == 0:
            terms = [
                jnp.dot(rows, pieces[j][...], preferred_element_type=jnp.float32)
                for j in (k, k + 1)
            ]
        else:
            both = jnp.concatenate([pieces[k][...], pieces[k + 1][...]], axis=1)
            term = jnp.dot(rows, both, preferred_element_type=jnp.float32)
            terms = [term[:, :size], term[:, size:]]
        for start, term in zip(starts, terms):
            columns = pl.ds(start, size)
            term = term.astype(jnp.bfloat16).astype(jnp.float32)
            done_ref[:, columns] = (ours_ref[:, columns].astype(jnp.float32) + term).astype(
                jnp.bfloat16
            )
        start = base + (jnp.bitwise_xor(slot_of(me, kind), change) // 2) * (2 * size)
        columns = pl.ds(pl.multiple_of(start, 256), 2 * size)
        out = pltpu.make_async_copy(
            done_ref.at[:, columns], out_hbm.at[:, columns], out_sems.at[k // 2]
        )
        out.start()
        leaving.append(out)
    for out in leaving:
        out.wait()


def on_device(
    query_latent,
    shared_latent,
    rotary_key,
    document_start,
    query_gain,
    shared_gain,
    content_weight,
    rotary_weight,
    key_weight,
    value_weight,
    output_weight,
):
    length, rank = shared_latent.shape
    count = lax.axis_size("sp")
    groups = lax.axis_size("tp")
    heads = key_weight.shape[1] // CONTENT
    model = output_weight.shape[1]
    me = lax.axis_index("sp")
    position = (me * length + jnp.arange(length, dtype=jnp.int32)).astype(jnp.float32)
    frequency = 1.0 / rope_theta ** (jnp.arange(0, ROTARY, 2, dtype=jnp.float32) / ROTARY)
    angles = frequency[:, None] * position[None, :]
    cosine, sine = jnp.cos(angles), jnp.sin(angles)

    plan = groups == 2 and count % 8 == 0 and model % 4096 == 0
    swap = [(0, 1), (1, 0)]
    cuts, base = [], 0
    for kind, share in KINDS if plan else ():
        size = share * model // 32
        cuts.append((base, size, kind))
        base += size * (8 if kind == "quad" else 4)

    packed_rows = length + length * ROTARY // rank
    if plan:
        parts = pl.pallas_call(
            functools.partial(cut_kernel, cuts, "sp"),
            out_shape=[
                jax.ShapeDtypeStruct((output_weight.shape[0], size), jnp.bfloat16)
                for _, size, _ in cuts
            ],
            in_specs=[hbm()],
            out_specs=[vmem()] * len(cuts),
            scratch_shapes=[pltpu.SemaphoreType.DMA((len(cuts),))],
            cost_estimate=pl.CostEstimate(
                flops=10**8, bytes_accessed=10**7, transcendentals=0
            ),
            compiler_params=grant(57),
            name="cut",
        )(output_weight)
    mine = pl.pallas_call(
        pack_kernel,
        out_shape=jax.ShapeDtypeStruct((packed_rows, rank), jnp.bfloat16),
        in_specs=[vmem()] * 5,
        out_specs=vmem(),
        cost_estimate=pl.CostEstimate(flops=2 * 10**10, bytes_accessed=2 * 10**7, transcendentals=0),
        compiler_params=grant(8),
        name="pack",
    )(shared_latent, rotary_key.T, shared_gain[None, :], cosine, sine)

    everyone = range(count)

    def hop(value, pairs):
        return lax.ppermute(value, "sp", pairs)

    core = [(i, i ^ 1) for i in everyone]
    ahead = [(i, i + GROUP) for i in everyone if i + GROUP < count]
    ahead_again = [(i, j) for i, j in ahead if i % GROUP > 0]
    up = [(i, i ^ 2) for i in everyone if i % GROUP < 2]
    down = [(i, i ^ 2) for i in everyone if i % GROUP >= 2]
    both = [(i, i ^ 2) for i in everyone]

    back1 = hop(mine, ahead)
    side0 = hop(mine, up)
    core0 = hop(mine, core)
    back2 = hop(back1, ahead_again)
    side1 = hop(back1, both)
    core1 = hop(back1, core)
    far0 = hop(side0, core)
    side2 = hop(back2, down)
    core2 = hop(back2, core)
    far1 = hop(side1, core)
    far2 = hop(side2, core)

    places, pieces = [], []
    if plan:
        over_z = [(i, i ^ 4) for i in everyone]
        over_y = [(i, i ^ 2) for i in everyone]
        for chunk, (base, size, kind) in enumerate(cuts):
            pulled = lax.ppermute(parts[chunk], "tp", swap)
            crossed = hop(pulled, over_y if kind == "y" else over_z)
            if kind == "quad":
                arrived = [(0, pulled), (4, crossed)]
                arrived += [(2, hop(pulled, over_y)), (6, hop(crossed, over_y))]
            else:
                arrived = [(0, pulled), (2, crossed)]
            for change, piece in arrived:
                places.append((base, size, kind, change))
                pieces.append(piece)
                places.append((base, size, kind, change + 1))
                pieces.append(hop(piece, core))

    latents = (query_latent, query_gain[None, :], content_weight, rotary_weight, value_weight, key_weight)
    queries, value_turned, stat, acc = pl.pallas_call(
        functools.partial(begin_kernel, "sp"),
        out_shape=(
            jax.ShapeDtypeStruct((heads, length, 2 * CONTENT), jnp.bfloat16),
            jax.ShapeDtypeStruct((heads * VALUE_DIM, rank), jnp.bfloat16),
            jax.ShapeDtypeStruct((2 * heads, length), jnp.float32),
            jax.ShapeDtypeStruct((heads, VALUE_DIM, length), jnp.float32),
        ),
        in_specs=[vmem()] * 10,
        out_specs=(vmem(),) * 4,
        scratch_shapes=work_area(heads, length),
        cost_estimate=pl.CostEstimate(flops=2 * 10**9, bytes_accessed=6 * 10**6, transcendentals=0),
        compiler_params=grant(14),
        name="begin",
    )(*latents, document_start[None, :], mine, cosine, sine)
    state = (stat, acc)

    def attend(state, pieces):
        stage = [place for place, _ in pieces]
        operands = [document_start, document_start[None, :], queries, key_weight, value_turned]
        operands += [array for _, array in pieces]
        aliases = {len(operands): 0, len(operands) + 1: 1}
        operands += list(state)
        return pl.pallas_call(
            functools.partial(attend_kernel, stage, "sp"),
            out_shape=(
                jax.ShapeDtypeStruct((2 * heads, length), jnp.float32),
                jax.ShapeDtypeStruct((heads, VALUE_DIM, length), jnp.float32),
            ),
            in_specs=[smem()] + [vmem()] * (len(operands) - 1),
            out_specs=(vmem(), vmem()),
            scratch_shapes=work_area(heads, length),
            input_output_aliases=aliases,
            cost_estimate=pl.CostEstimate(
                flops=10**9 * len(stage), bytes_accessed=5 * 10**6, transcendentals=0
            ),
            compiler_params=grant(18),
        )(*operands)

    state = attend(state, [(at(1, 0), core0), (at(2, 0), side0), (at(0, 4), back1)])
    state = attend(state, [(at(3, 0), far0), (at(1, 4), core1), (at(2, 4), side1)])
    state = attend(state, [(at(3, 4), far1), (at(1, 8), core2)])
    state = attend(state, [(at(2, 8), side2), (at(3, 8), far2)])

    attended = pl.pallas_call(
        functools.partial(finish_kernel, heads),
        out_shape=jax.ShapeDtypeStruct((length, heads * VALUE_DIM), jnp.bfloat16),
        in_specs=[vmem()] * 2,
        out_specs=vmem(),
        cost_estimate=pl.CostEstimate(flops=10**8, bytes_accessed=10**6, transcendentals=0),
        compiler_params=grant(8),
        name="finish",
    )(*state)

    if not plan:
        mixed = jnp.dot(attended, output_weight, preferred_element_type=jnp.float32)
        return lax.psum(mixed.astype(jnp.bfloat16), "tp")

    theirs = lax.ppermute(attended, "tp", swap)
    ours = pl.pallas_call(
        project_kernel,
        out_shape=jax.ShapeDtypeStruct((length, model), jnp.bfloat16),
        in_specs=[vmem()] * 2,
        out_specs=vmem(),
        cost_estimate=pl.CostEstimate(
            flops=2 * 10**9, bytes_accessed=10**7, transcendentals=0
        ),
        compiler_params=grant(14),
        name="ours",
    )(attended, output_weight)
    mixed = None
    for low, high in ((0, EARLY), (EARLY, len(pieces))):
        operands = [theirs, ours, *pieces[low:high]]
        aliases = {}
        if mixed is not None:
            aliases = {len(operands): 0}
            operands.append(mixed)
        mixed = pl.pallas_call(
            functools.partial(combine_kernel, places[low:high], "sp"),
            out_shape=jax.ShapeDtypeStruct((length, model), jnp.bfloat16),
            in_specs=[vmem()] * (2 + high - low)
            + [hbm()] * (len(operands) - 2 - high + low),
            out_specs=hbm(),
            scratch_shapes=[
                pltpu.VMEM((length, model), jnp.bfloat16),
                pltpu.SemaphoreType.DMA(((high - low) // 2,)),
            ],
            input_output_aliases=aliases,
            cost_estimate=pl.CostEstimate(flops=10**9, bytes_accessed=5 * 10**6, transcendentals=0),
            compiler_params=grant(14),
        )(*operands)
    return mixed


def solution(mesh):
    return jax.shard_map(
        on_device,
        mesh=mesh,
        in_specs=(
            P("sp", None),
            P("sp", None),
            P("sp", None),
            P("sp"),
            P(),
            P(),
            P(None, "tp"),
            P(None, "tp"),
            P(None, "tp"),
            P(None, "tp"),
            P("tp", None),
        ),
        out_specs=P("sp", None),
        check_vma=False,
    )
```

```python
import functools

import jax
import jax.numpy as jnp
from jax import lax
from jax.experimental import pallas as pl
from jax.experimental.pallas import tpu as pltpu
from jax.sharding import PartitionSpec as P

CONTENT = 128
ROTARY = 64
VALUE_DIM = 128
GROUP = 4
KINDS = (("quad", 1), ("z", 2), ("y", 2), ("z", 1), ("z", 1))

norm_eps = 1e-06
rope_theta = 10000.0
masked_score = -1e30
LOG2E = 1.4426950408889634


def vmem():
    return pl.BlockSpec(memory_space=pltpu.VMEM)


def grant(mebibytes):
    return pltpu.CompilerParams(vmem_limit_bytes=mebibytes * 2**20)


def hbm():
    return pl.BlockSpec(memory_space=pltpu.HBM)


def smem():
    return pl.BlockSpec(memory_space=pltpu.SMEM)


def normed(latent, gain):
    entries = latent.astype(jnp.float32)
    scale = lax.rsqrt(jnp.mean(entries * entries, axis=-1, keepdims=True) + norm_eps)
    return (entries * scale * gain).astype(jnp.bfloat16)


def swap_halves(x):
    width = x.shape[-1]
    half = ROTARY // 2
    lane = lax.broadcasted_iota(jnp.int32, x.shape, x.ndim - 1)
    ahead = pltpu.roll(x, width - half, x.ndim - 1)
    behind = pltpu.roll(x, half, x.ndim - 1)
    return jnp.where(lane % ROTARY < half, ahead, behind)


def load(pairs, sems):
    copies = [pltpu.make_async_copy(src, dst, sems.at[k]) for k, (src, dst) in enumerate(pairs)]
    for copy in copies:
        copy.start()
    return copies


def cut_kernel(cuts, axis, weight_hbm, *refs):
    parts, sems = refs[:-1], refs[-1]
    me = lax.axis_index(axis)
    pairs = []
    for (base, size, kind), part_ref in zip(cuts, parts):
        start = pl.multiple_of(base + slot_of(me, kind) * size, 128)
        pairs.append((weight_hbm.at[:, pl.ds(start, size)], part_ref))
    for copy in load(pairs, sems):
        copy.wait()


def pack_kernel(shared_ref, rotary_ref, gain_ref, cos_ref, sin_ref, out_ref):
    length, rank = shared_ref.shape
    half = ROTARY // 2
    key = rotary_ref[...].astype(jnp.float32)
    low, high = key[:half], key[half:]
    cosine, sine = cos_ref[...], sin_ref[...]
    turned = jnp.concatenate([low * cosine - high * sine, low * sine + high * cosine], axis=0)
    turned = jnp.concatenate([turned, turned], axis=0).T
    rows = length * ROTARY // rank
    lane = lax.broadcasted_iota(jnp.int32, (rows, 2 * ROTARY), 1)
    for pair in range(rank // (2 * ROTARY)):
        low = turned[(2 * pair) * rows : (2 * pair + 1) * rows]
        high = turned[(2 * pair + 1) * rows : (2 * pair + 2) * rows]
        out_ref[length:, pair * 2 * ROTARY : (pair + 1) * 2 * ROTARY] = jnp.where(
            lane < ROTARY, low, high
        ).astype(jnp.bfloat16)
    out_ref[0:length, :] = normed(shared_ref[...], gain_ref[...])


def begin_kernel(axis, *refs):
    latent_ref, gain_ref, content_ref, rotary_ref, value_ref, key_ref = refs[:6]
    starts_ref, block_ref, cos_ref, sin_ref = refs[6:10]
    query_ref, turned_value_ref, stat_ref, acc_ref = refs[10:14]
    scratch = refs[14:]
    cos4 = jnp.concatenate([cos_ref[...]] * 4, axis=0).T
    sin4 = jnp.concatenate([-sin_ref[...], sin_ref[...]] * 2, axis=0).T
    rows = normed(latent_ref[...], gain_ref[...])
    content = jnp.dot(rows, content_ref[...], preferred_element_type=jnp.float32)
    for head in range(query_ref.shape[0]):
        query_ref[head, :, 0:CONTENT] = content[:, head * CONTENT : (head + 1) * CONTENT].astype(
            jnp.bfloat16
        )
    raw = jnp.dot(rows, rotary_ref[...], preferred_element_type=jnp.float32)
    lane = lax.broadcasted_iota(jnp.int32, (rows.shape[0], 2 * ROTARY), 1)
    for pair in range(query_ref.shape[0] // 2):
        piece = raw[:, pair * 2 * ROTARY : (pair + 1) * 2 * ROTARY]
        turned = piece * cos4 + swap_halves(piece) * sin4
        for side in range(2):
            own = (lane < ROTARY) if side == 0 else (lane >= ROTARY)
            query_ref[2 * pair + side, :, CONTENT:] = jnp.where(own, turned, 0.0).astype(
                jnp.bfloat16
            )
    turned_value_ref[...] = value_ref[...].T
    me = lax.axis_index(axis)
    absorb(
        me, me, True, block_ref, starts_ref, query_ref, key_ref, turned_value_ref, stat_ref, acc_ref, *scratch
    )


def absorb(
    me, block, own, block_ref, starts_ref, query_ref, key_ref, value_ref, stat_ref, acc_ref,
    bias_ref, keys_ref, values_ref, scores_ref, weights_ref,
):
    heads, length = query_ref.shape[0], query_ref.shape[1]
    rank = key_ref.shape[0]
    scale = (CONTENT + ROTARY) ** (-0.5) * LOG2E
    shared = block_ref[0:length, :]
    keys_ref[...] = jnp.dot(shared, key_ref[...], preferred_element_type=jnp.float32).astype(
        jnp.bfloat16
    )
    values_ref[...] = lax.dot_general(
        value_ref[...], shared, (((1,), (1,)), ((), ())), preferred_element_type=jnp.float32
    ).astype(jnp.bfloat16)
    rows = length * ROTARY // rank
    pieces = []
    lane = lax.broadcasted_iota(jnp.int32, (rows, 2 * ROTARY), 1)
    for pair in range(rank // (2 * ROTARY)):
        tile = block_ref[length:, pair * 2 * ROTARY : (pair + 1) * 2 * ROTARY].astype(jnp.float32)
        other = pltpu.roll(tile, ROTARY, 1)
        pieces.append(jnp.where(lane < ROTARY, tile, other))
        pieces.append(jnp.where(lane < ROTARY, other, tile))
    turned = jnp.concatenate(pieces, axis=0).astype(jnp.bfloat16)
    key_place = block * length + lax.broadcasted_iota(jnp.int32, (length, length), 0)
    visible = key_place >= starts_ref[...]
    if own:
        query_place = me * length + lax.broadcasted_iota(jnp.int32, (length, length), 1)
        visible = visible & (key_place <= query_place)
    bias_ref[...] = jnp.where(visible, 0.0, masked_score)
    tops, factors = [], []
    for head in range(heads):
        keys = jnp.concatenate([keys_ref[:, head * CONTENT : (head + 1) * CONTENT], turned], axis=1)
        scores = lax.dot_general(
            keys, query_ref[head], (((1,), (1,)), ((), ())), preferred_element_type=jnp.float32
        )
        scores = scores * scale + bias_ref[...]
        scores_ref[head] = scores
        highest = jnp.max(scores, axis=0, keepdims=True)
        if not own:
            highest = jnp.maximum(highest, stat_ref[head : head + 1, :])
        tops.append(highest)
    piece = 64
    for head in range(heads):
        total = jnp.zeros((1, length), jnp.float32)
        for row in range(0, length, piece):
            weights = jnp.exp2(scores_ref[head, row : row + piece, :] - tops[head])
            total = total + jnp.sum(weights, axis=0, keepdims=True)
            weights_ref[head, row : row + piece, :] = weights.astype(jnp.bfloat16)
        if not own:
            factor = jnp.exp2(stat_ref[head : head + 1, :] - tops[head])
            factors.append(factor)
            total = total + stat_ref[heads + head : heads + head + 1, :] * factor
        stat_ref[head : head + 1, :] = tops[head]
        stat_ref[heads + head : heads + head + 1, :] = total
    for head in range(heads):
        summed = jnp.dot(
            values_ref[head * VALUE_DIM : (head + 1) * VALUE_DIM, :],
            weights_ref[head],
            preferred_element_type=jnp.float32,
        )
        acc_ref[head] = summed if own else acc_ref[head] * factors[head] + summed


def work_area(heads, length):
    return [
        pltpu.VMEM((length, length), jnp.float32),
        pltpu.VMEM((length, heads * CONTENT), jnp.bfloat16),
        pltpu.VMEM((heads * VALUE_DIM, length), jnp.bfloat16),
        pltpu.VMEM((heads, length, length), jnp.float32),
        pltpu.VMEM((heads, length, length), jnp.bfloat16),
    ]


def attend_kernel(places, axis, *refs):
    count = len(places)
    starts_smem, starts_ref, query_ref, key_ref, value_ref = refs[:5]
    blocks, refs = refs[5 : 5 + count], refs[5 + count :]
    old_stat, old_acc, stat_ref, acc_ref = refs[:4]
    scratch = refs[4:]
    length = query_ref.shape[1]
    me = lax.axis_index(axis)
    stat_ref[...] = old_stat[...]
    acc_ref[...] = old_acc[...]
    for place_of, block_ref in zip(places, blocks):
        block = place_of(me)
        needed = (block >= 0) & (block <= me) & ((block + 1) * length - 1 >= starts_smem[0])
        pl.when(needed)(
            functools.partial(
                absorb, me, block, False, block_ref, starts_ref, query_ref, key_ref, value_ref,
                stat_ref, acc_ref, *scratch,
            )
        )


def at(flip, back):
    def place(me):
        return jnp.bitwise_xor(me, flip) - back if back else jnp.bitwise_xor(me, flip)

    return place


def finish_kernel(heads, stat_ref, acc_ref, out_ref):
    for head in range(heads):
        ratio = acc_ref[head] / stat_ref[heads + head : heads + head + 1, :]
        out_ref[:, head * VALUE_DIM : (head + 1) * VALUE_DIM] = ratio.T.astype(jnp.bfloat16)


def project_kernel(rows_ref, weight_ref, out_ref):
    tile = 512

    @pl.loop(0, weight_ref.shape[1] // tile)
    def _(step):
        columns = pl.ds(pl.multiple_of(step * tile, tile), tile)
        out_ref[:, columns] = jnp.dot(
            rows_ref[...], weight_ref[:, columns], preferred_element_type=jnp.float32
        ).astype(jnp.bfloat16)


def slot_of(me, kind):
    if kind == "quad":
        return jnp.bitwise_and(me, 7)
    bit = 2 if kind == "z" else 1
    return jnp.bitwise_and(lax.shift_right_logical(me, bit), 1) * 2 + jnp.bitwise_and(me, 1)


def combine_kernel(places, axis, rows_ref, ours_ref, *refs):
    me = lax.axis_index(axis)
    count = len(places)
    pieces, (out_hbm, done_ref, out_sems) = refs[:count], refs[-3:]
    rows = rows_ref[...]
    leaving = []
    for k in range(0, count, 2):
        base, size, kind, change = places[k]
        starts = [
            pl.multiple_of(base + jnp.bitwise_xor(slot_of(me, kind), flip) * size, 128)
            for flip in (change, change + 1)
        ]
        if size % 256 == 0:
            terms = [
                jnp.dot(rows, pieces[j][...], preferred_element_type=jnp.float32)
                for j in (k, k + 1)
            ]
        else:
            both = jnp.concatenate([pieces[k][...], pieces[k + 1][...]], axis=1)
            term = jnp.dot(rows, both, preferred_element_type=jnp.float32)
            terms = [term[:, :size], term[:, size:]]
        for start, term in zip(starts, terms):
            columns = pl.ds(start, size)
            term = term.astype(jnp.bfloat16).astype(jnp.float32)
            done_ref[:, columns] = (ours_ref[:, columns].astype(jnp.float32) + term).astype(
                jnp.bfloat16
            )
        start = base + (jnp.bitwise_xor(slot_of(me, kind), change) // 2) * (2 * size)
        columns = pl.ds(pl.multiple_of(start, 256), 2 * size)
        out = pltpu.make_async_copy(
            done_ref.at[:, columns], out_hbm.at[:, columns], out_sems.at[k // 2]
        )
        out.start()
        leaving.append(out)
    for out in leaving:
        out.wait()


def on_device(
    query_latent,
    shared_latent,
    rotary_key,
    document_start,
    query_gain,
    shared_gain,
    content_weight,
    rotary_weight,
    key_weight,
    value_weight,
    output_weight,
):
    length, rank = shared_latent.shape
    count = lax.axis_size("sp")
    groups = lax.axis_size("tp")
    heads = key_weight.shape[1] // CONTENT
    model = output_weight.shape[1]
    me = lax.axis_index("sp")
    position = (me * length + jnp.arange(length, dtype=jnp.int32)).astype(jnp.float32)
    frequency = 1.0 / rope_theta ** (jnp.arange(0, ROTARY, 2, dtype=jnp.float32) / ROTARY)
    angles = frequency[:, None] * position[None, :]
    cosine, sine = jnp.cos(angles), jnp.sin(angles)

    plan = groups == 2 and count % 8 == 0 and model % 4096 == 0
    swap = [(0, 1), (1, 0)]
    cuts, base = [], 0
    for kind, share in KINDS if plan else ():
        size = share * model // 32
        cuts.append((base, size, kind))
        base += size * (8 if kind == "quad" else 4)

    packed_rows = length + length * ROTARY // rank
    if plan:
        parts = pl.pallas_call(
            functools.partial(cut_kernel, cuts, "sp"),
            out_shape=[
                jax.ShapeDtypeStruct((output_weight.shape[0], size), jnp.bfloat16)
                for _, size, _ in cuts
            ],
            in_specs=[hbm()],
            out_specs=[vmem()] * len(cuts),
            scratch_shapes=[pltpu.SemaphoreType.DMA((len(cuts),))],
            cost_estimate=pl.CostEstimate(
                flops=10**8, bytes_accessed=10**7, transcendentals=0
            ),
            compiler_params=grant(57),
            name="cut",
        )(output_weight)
    mine = pl.pallas_call(
        pack_kernel,
        out_shape=jax.ShapeDtypeStruct((packed_rows, rank), jnp.bfloat16),
        in_specs=[vmem()] * 5,
        out_specs=vmem(),
        cost_estimate=pl.CostEstimate(flops=2 * 10**10, bytes_accessed=2 * 10**7, transcendentals=0),
        compiler_params=grant(8),
        name="pack",
    )(shared_latent, rotary_key.T, shared_gain[None, :], cosine, sine)

    everyone = range(count)

    def hop(value, pairs):
        return lax.ppermute(value, "sp", pairs)

    core = [(i, i ^ 1) for i in everyone]
    ahead = [(i, i + GROUP) for i in everyone if i + GROUP < count]
    ahead_again = [(i, j) for i, j in ahead if i % GROUP > 0]
    up = [(i, i ^ 2) for i in everyone if i % GROUP < 2]
    down = [(i, i ^ 2) for i in everyone if i % GROUP >= 2]
    both = [(i, i ^ 2) for i in everyone]

    back1 = hop(mine, ahead)
    side0 = hop(mine, up)
    core0 = hop(mine, core)
    back2 = hop(back1, ahead_again)
    side1 = hop(back1, both)
    core1 = hop(back1, core)
    far0 = hop(side0, core)
    side2 = hop(back2, down)
    core2 = hop(back2, core)
    far1 = hop(side1, core)
    far2 = hop(side2, core)

    places, pieces = [], []
    if plan:
        over_z = [(i, i ^ 4) for i in everyone]
        over_y = [(i, i ^ 2) for i in everyone]
        for chunk, (base, size, kind) in enumerate(cuts):
            pulled = lax.ppermute(parts[chunk], "tp", swap)
            crossed = hop(pulled, over_y if kind == "y" else over_z)
            if kind == "quad":
                arrived = [(0, pulled), (4, crossed)]
                arrived += [(2, hop(pulled, over_y)), (6, hop(crossed, over_y))]
            else:
                arrived = [(0, pulled), (2, crossed)]
            for change, piece in arrived:
                places.append((base, size, kind, change))
                pieces.append(piece)
                places.append((base, size, kind, change + 1))
                pieces.append(hop(piece, core))

    latents = (query_latent, query_gain[None, :], content_weight, rotary_weight, value_weight, key_weight)
    queries, value_turned, stat, acc = pl.pallas_call(
        functools.partial(begin_kernel, "sp"),
        out_shape=(
            jax.ShapeDtypeStruct((heads, length, 2 * CONTENT), jnp.bfloat16),
            jax.ShapeDtypeStruct((heads * VALUE_DIM, rank), jnp.bfloat16),
            jax.ShapeDtypeStruct((2 * heads, length), jnp.float32),
            jax.ShapeDtypeStruct((heads, VALUE_DIM, length), jnp.float32),
        ),
        in_specs=[vmem()] * 10,
        out_specs=(vmem(),) * 4,
        scratch_shapes=work_area(heads, length),
        cost_estimate=pl.CostEstimate(flops=2 * 10**9, bytes_accessed=6 * 10**6, transcendentals=0),
        compiler_params=grant(14),
        name="begin",
    )(*latents, document_start[None, :], mine, cosine, sine)
    state = (stat, acc)

    def attend(state, pieces):
        stage = [place for place, _ in pieces]
        operands = [document_start, document_start[None, :], queries, key_weight, value_turned]
        operands += [array for _, array in pieces]
        aliases = {len(operands): 0, len(operands) + 1: 1}
        operands += list(state)
        return pl.pallas_call(
            functools.partial(attend_kernel, stage, "sp"),
            out_shape=(
                jax.ShapeDtypeStruct((2 * heads, length), jnp.float32),
                jax.ShapeDtypeStruct((heads, VALUE_DIM, length), jnp.float32),
            ),
            in_specs=[smem()] + [vmem()] * (len(operands) - 1),
            out_specs=(vmem(), vmem()),
            scratch_shapes=work_area(heads, length),
            input_output_aliases=aliases,
            cost_estimate=pl.CostEstimate(
                flops=10**9 * len(stage), bytes_accessed=5 * 10**6, transcendentals=0
            ),
            compiler_params=grant(18),
        )(*operands)

    state = attend(state, [(at(1, 0), core0), (at(2, 0), side0), (at(0, 4), back1)])
    state = attend(state, [(at(3, 0), far0), (at(1, 4), core1), (at(2, 4), side1)])
    state = attend(state, [(at(3, 4), far1), (at(1, 8), core2)])
    state = attend(state, [(at(2, 8), side2), (at(3, 8), far2)])

    attended = pl.pallas_call(
        functools.partial(finish_kernel, heads),
        out_shape=jax.ShapeDtypeStruct((length, heads * VALUE_DIM), jnp.bfloat16),
        in_specs=[vmem()] * 2,
        out_specs=vmem(),
        cost_estimate=pl.CostEstimate(flops=10**8, bytes_accessed=10**6, transcendentals=0),
        compiler_params=grant(8),
        name="finish",
    )(*state)

    if not plan:
        mixed = jnp.dot(attended, output_weight, preferred_element_type=jnp.float32)
        return lax.psum(mixed.astype(jnp.bfloat16), "tp")

    theirs = lax.ppermute(attended, "tp", swap)
    ours = pl.pallas_call(
        project_kernel,
        out_shape=jax.ShapeDtypeStruct((length, model), jnp.bfloat16),
        in_specs=[vmem()] * 2,
        out_specs=vmem(),
        cost_estimate=pl.CostEstimate(
            flops=2 * 10**9, bytes_accessed=10**7, transcendentals=0
        ),
        compiler_params=grant(14),
        name="ours",
    )(attended, output_weight)
    mixed = None
    for low, high in ((0, len(pieces)),):
        operands = [theirs, ours, *pieces[low:high]]
        aliases = {}
        if mixed is not None:
            aliases = {len(operands): 0}
            operands.append(mixed)
        mixed = pl.pallas_call(
            functools.partial(combine_kernel, places[low:high], "sp"),
            out_shape=jax.ShapeDtypeStruct((length, model), jnp.bfloat16),
            in_specs=[vmem()] * (2 + high - low)
            + [hbm()] * (len(operands) - 2 - high + low),
            out_specs=hbm(),
            scratch_shapes=[
                pltpu.VMEM((length, model), jnp.bfloat16),
                pltpu.SemaphoreType.DMA(((high - low) // 2,)),
            ],
            input_output_aliases=aliases,
            cost_estimate=pl.CostEstimate(flops=10**9, bytes_accessed=5 * 10**6, transcendentals=0),
            compiler_params=grant(14),
        )(*operands)
    return mixed


def solution(mesh):
    return jax.shard_map(
        on_device,
        mesh=mesh,
        in_specs=(
            P("sp", None),
            P("sp", None),
            P("sp", None),
            P("sp"),
            P(),
            P(),
            P(None, "tp"),
            P(None, "tp"),
            P(None, "tp"),
            P(None, "tp"),
            P("tp", None),
        ),
        out_specs=P("sp", None),
        check_vma=False,
    )
```
